128 devices in a mesh: ep: 64 (over z, y, x), tp: 2 (over core).
Axes of the slice: x: 4, y: 4, z: 4, core: 2. Of those that a mesh axis runs over, the one named last changes fastest.
Arguments:
- tokens: bfloat16 [1536, 2048], P('ep'), may hold values from -6 to 6
- attn_gain: float32 [2048], replicated, may hold values from 0.1 to 1.9
- w_query: bfloat16 [2048, 1024], P(None, 'tp'), may hold values from -0.125 to 0.125
- w_key: bfloat16 [2048, 1024], P(None, 'tp'), may hold values from -0.125 to 0.125
- w_value: bfloat16 [2048, 1024], P(None, 'tp'), may hold values from -0.125 to 0.125
- w_zgate: bfloat16 [2048, 1024], P(None, 'tp'), may hold values from -0.125 to 0.125
- w_decay: bfloat16 [2048, 8], P(None, 'tp'), may hold values from -0.125 to 0.125
- w_beta: bfloat16 [2048, 8], P(None, 'tp'), may hold values from -0.125 to 0.125
- decay_rate: float32 [8], P('tp'), may hold values from 0.05 to 2
- decay_bias: float32 [8], P('tp'), may hold values from -3 to 3
- state: float32 [1536, 8, 128, 128], P('ep', 'tp'), may hold values from -2 to 2
- out_gain: float32 [128], replicated, may hold values from 0.1 to 1.9
- w_out: bfloat16 [1024, 2048], P('tp'), may hold values from -0.1875 to 0.1875
- ffn_gain: float32 [2048], replicated, may hold values from 0.1 to 1.9
- expert_gate: bfloat16 [64, 2048, 512], P('ep', None, 'tp'), may hold values from -0.125 to 0.125
- expert_up: bfloat16 [64, 2048, 512], P('ep', None, 'tp'), may hold values from -0.125 to 0.125
- expert_down: bfloat16 [64, 512, 2048], P('ep', 'tp'), may hold values from -0.25 to 0.25
- routes: int32 [1536, 2], P('ep'), may hold values from 0 to 63, all different within a row; in each aligned block of 24 rows (0 to 23, 24 to 47, ...) at most 2 rows name the same one
- route_weight: float32 [1536, 2], P('ep'), may hold values from 0.2 to 1
Outputs:
- layer_out: bfloat16 [1536, 2048], P('ep', 'tp')
- new_state: float32 [1536, 8, 128, 128], P('ep', 'tp')
The draws below stay inside these ranges and needn't reach their ends.
Inputs may be any that keep to these rules, and one draw needn't show every extreme that they name: `routes`: the 2 entries of a row differ. Among the rows of one index of ep (aligned blocks of 24 rows) no expert is named more than 2 times, a bound that some block reaches.
All inputs are finite; a program needn't handle non-finite values.
Results may differ from the reference program's by a relative error of at most 0.014.
Values may be sent and summed in bfloat16 or wider, within the bound.
A program may use at most 128 MiB of HBM per device.

```python
import math
import jax
import jax.numpy as jnp
import numpy as np
from jax import lax

D = 2048
HEADS = 8
HEAD_DIM = 128
FF_EXP = 512
TOP_K = 2
SEQS_DEV = 24
SEQS = 1536
EXPERTS = 64
CAP = 2
N_EP = 64
N_TP = 2


def levels(stream_key, shape, cuts, least, top_value):
    def one(position, blocks):
        draws = jax.random.uniform(jax.random.fold_in(jax.random.fold_in(stream_key, 6), position), (blocks,), jnp.float32, least / len(cuts), top_value / len(cuts))
        return jnp.repeat(jnp.exp(draws), shape[position] // blocks).reshape((-1,) + (1,) * (len(shape) - position - 1))

    factor_of = one(*cuts[0])
    for cut in cuts[1:]:
        factor_of = factor_of * one(*cut)
    return factor_of


def deal_out(rng, own, number, rows, count, top, reach, lean):
    sequence = jax.random.permutation(rng, count)
    heavy_load, ordinary = shares(count, rows * top, reach, lean, True), shares(count, rows * top, reach, lean, False)
    places = jnp.arange(count)

    def named(tallies, rotation):
        used = int((tallies > 0).sum())
        fixed = max(1, used // 4)
        moved = fixed + (places - fixed + rotation * (used - fixed)) % max(1, count - fixed)
        return jnp.zeros((count,), jnp.int32).at[sequence[jnp.where(places < fixed, places, moved)]].set(jnp.asarray(tallies, jnp.int32))

    tallies = jnp.where(number % 4 == 0, named(heavy_load, number // 4), named(ordinary, number - number // 4 - 1))
    mixed = jax.random.permutation(jax.random.fold_in(own, 3), count)
    giver, sink = mixed[0:count // 2 * 2:2], mixed[1:count // 2 * 2:2]
    slack = jnp.minimum(tallies[giver] - 1, reach - tallies[sink]) // 2
    slack = jnp.where((giver == sequence[0]) | (sink == sequence[0]) | (tallies[sink] == 0), 0, jnp.maximum(slack, 0))
    moved = jax.random.randint(jax.random.fold_in(own, 4), (count // 2,), 0, 1 << 20) % (slack + 1)
    tallies = tallies.at[giver].add(-moved).at[sink].add(moved)
    items = jnp.searchsorted(jnp.cumsum(tallies), jnp.arange(rows * top), side="right").astype(jnp.int32)
    listing = items.reshape(top, rows).T
    listing = listing[jax.random.permutation(jax.random.fold_in(own, 1), rows)]
    rotation = jax.random.randint(jax.random.fold_in(own, 2), (rows, 1), 0, top)
    return jnp.take_along_axis(listing, (jnp.arange(top)[None, :] + rotation) % top, axis=1)


def shares(amount, total, reach, slope, full):
    weights = [(1 << 20) // math.isqrt(rank ** slope) + 1 for rank in range(1, amount + 1)]
    largest = reach if full else min(reach, max(-(-total // amount), total * weights[0] // sum(weights)))
    least = 1 if total - largest >= amount - 1 else 0
    counts, rest = [largest] + [least] * (amount - 1), total - largest - least * (amount - 1)
    while rest > 0:
        movable = [i for i in range(1, amount) if counts[i] < largest] or [i for i in range(1, amount) if counts[i] < reach]
        pool, budget = sum([weights[i] for i in movable]), rest
        for i in movable:
            extra = min(reach - counts[i], max(1, budget * weights[i] // pool), rest)
            counts[i] = counts[i] + extra
            rest = rest - extra
    return np.array(counts)


def normal_values(stream_key, dims, width, limit, shards=(), kind=jnp.bfloat16):
    entries = width * jax.random.normal(stream_key, dims, jnp.float32)
    if shards:
        entries = entries * levels(stream_key, dims, shards, -0.22, 0.18)
    return jnp.clip(entries, -limit, limit).astype(kind)


def setup_inputs(seed: int = 0) -> dict:
    streams_of = jax.random.split(jax.random.key(seed), 20)
    tokens = normal_values(streams_of[0], (SEQS, D), 1.0, 6.0, ((0, 64),))
    attn_gain = jnp.clip(1.0 + 0.18 * jax.random.normal(streams_of[1], (D,), jnp.float32), 0.1, 1.9)
    w_query = normal_values(streams_of[2], (D, HEADS * HEAD_DIM), D ** -0.5, 0.125, ((1, 2),))
    w_key = normal_values(streams_of[3], (D, HEADS * HEAD_DIM), D ** -0.5, 0.125, ((1, 2),))
    w_value = normal_values(streams_of[4], (D, HEADS * HEAD_DIM), D ** -0.5, 0.125, ((1, 2),))
    w_zgate = normal_values(streams_of[5], (D, HEADS * HEAD_DIM), D ** -0.5, 0.125, ((1, 2),))
    w_decay = normal_values(streams_of[6], (D, HEADS), D ** -0.5, 0.125, ((1, 2),))
    w_beta = normal_values(streams_of[7], (D, HEADS), D ** -0.5, 0.125, ((1, 2),))
    decay_rate = jnp.clip(jnp.exp(math.log(2.0) - 3.6888794 * jax.random.uniform(streams_of[8], (HEADS,), jnp.float32) ** levels(streams_of[8], (HEADS,), ((0, 2),), -0.2, 0.2)), 0.05, 2.0)
    decay_bias = normal_values(streams_of[9], (HEADS,), 1.0, 3.0, ((0, 2),), jnp.float32)
    state = normal_values(streams_of[10], (SEQS, HEADS, HEAD_DIM, HEAD_DIM), 0.3, 2.0, ((0, 64), (1, 2)), jnp.float32)
    out_gain = jnp.clip(1.0 + 0.18 * jax.random.normal(streams_of[11], (HEAD_DIM,), jnp.float32), 0.1, 1.9)
    w_out = normal_values(streams_of[12], (HEADS * HEAD_DIM, D), (HEADS * HEAD_DIM) ** -0.5, 0.1875, ((0, 2),))
    ffn_gain = jnp.clip(1.0 + 0.18 * jax.random.normal(streams_of[13], (D,), jnp.float32), 0.1, 1.9)
    expert_gate = normal_values(streams_of[14], (EXPERTS, D, FF_EXP), D ** -0.5, 0.125, ((0, 64), (2, 2)))
    expert_up = normal_values(streams_of[15], (EXPERTS, D, FF_EXP), D ** -0.5, 0.125, ((0, 64), (2, 2)))
    expert_down = normal_values(streams_of[16], (EXPERTS, FF_EXP, D), FF_EXP ** -0.5, 0.25, ((0, 64), (1, 2)))
    routes_keys = jax.random.split(jax.random.fold_in(streams_of[17], 1), SEQS // SEQS_DEV)
    routes_turns = jax.random.permutation(jax.random.fold_in(streams_of[17], 3), SEQS // SEQS_DEV)
    routes = jax.vmap(lambda own, number: deal_out(jax.random.fold_in(streams_of[17], 2), own, number, SEQS_DEV, EXPERTS, TOP_K, CAP, 2))(routes_keys, routes_turns).reshape((SEQS, TOP_K))
    route_weight = jnp.clip(0.2 + 0.8 * jax.random.uniform(streams_of[18], (SEQS, TOP_K), jnp.float32) ** levels(streams_of[18], (SEQS, TOP_K), ((0, 64),), -0.2, 0.2), 0.2, 1.0)
    return dict(tokens=tokens, attn_gain=attn_gain, w_query=w_query, w_key=w_key, w_value=w_value, w_zgate=w_zgate, w_decay=w_decay, w_beta=w_beta, decay_rate=decay_rate, decay_bias=decay_bias, state=state, out_gain=out_gain, w_out=w_out, ffn_gain=ffn_gain, expert_gate=expert_gate, expert_up=expert_up, expert_down=expert_down, routes=routes, route_weight=route_weight)


EPS = 1e-06

def rms_scale(rows, gain):
    return rows * lax.rsqrt(lax.optimization_barrier(jnp.mean(rows * rows, axis=-1, keepdims=True)) + EPS) * gain

def unit_rows(rows):
    return rows * lax.rsqrt(lax.optimization_barrier(jnp.sum(rows * rows, axis=-1, keepdims=True)) + EPS)

def mixer_block(args):
    normed, w_query, w_key, w_value, w_zgate, w_decay, w_beta, decay_rate, decay_bias, state, out_gain = args
    seqs = normed.shape[0]

    def project(weight):
        return jnp.dot(normed, weight, preferred_element_type=jnp.float32).astype(jnp.bfloat16)

    def heads_of(raw):
        return raw.reshape(seqs, HEADS, HEAD_DIM).astype(jnp.float32)
    query = unit_rows(jax.nn.silu(heads_of(project(w_query)))) * HEAD_DIM ** (-0.5)
    key = unit_rows(jax.nn.silu(heads_of(project(w_key))))
    value = jax.nn.silu(heads_of(project(w_value)))
    zmul = jax.nn.silu(heads_of(project(w_zgate)))
    fade = jnp.exp(-decay_rate * jax.nn.softplus(project(w_decay).astype(jnp.float32) + decay_bias))
    beta = jax.nn.sigmoid(project(w_beta).astype(jnp.float32))
    predicted = jnp.einsum('shkv,shk->shv', state, key, precision=lax.Precision.HIGHEST)
    written = beta[..., None] * (value - fade[..., None] * predicted)
    updated = fade[..., None, None] * state + key[..., :, None] * written[..., None, :]
    read = jnp.einsum('shkv,shk->shv', updated, query, precision=lax.Precision.HIGHEST)
    heads_out = (rms_scale(read, out_gain) * zmul).astype(jnp.bfloat16)
    return (heads_out.reshape(seqs, HEADS * HEAD_DIM), updated)

def reference(tokens, attn_gain, w_query, w_key, w_value, w_zgate, w_decay, w_beta, decay_rate, decay_bias, state, out_gain, w_out, ffn_gain, expert_gate, expert_up, expert_down, routes, route_weight):
    resid_in = tokens.astype(jnp.float32)
    normed = rms_scale(resid_in, attn_gain).astype(jnp.bfloat16)

    def one_block(args):
        block_rows, block_state = args
        return mixer_block((block_rows, w_query, w_key, w_value, w_zgate, w_decay, w_beta, decay_rate, decay_bias, block_state, out_gain))
    heads_out, new_state = lax.map(one_block, (normed.reshape(N_EP, SEQS_DEV, D), state.reshape(N_EP, SEQS_DEV, HEADS, HEAD_DIM, HEAD_DIM)))
    heads_out = heads_out.reshape(SEQS, HEADS * HEAD_DIM)
    new_state = new_state.reshape(SEQS, HEADS, HEAD_DIM, HEAD_DIM)
    group = HEADS * HEAD_DIM // N_TP
    mixed = jnp.zeros((SEQS, D), jnp.float32)
    for part in range(N_TP):
        term = jnp.dot(heads_out[:, part * group:(part + 1) * group], w_out[part * group:(part + 1) * group], preferred_element_type=jnp.float32)
        mixed = mixed + term.astype(jnp.bfloat16).astype(jnp.float32)
    resid = resid_in + mixed
    moe_in = rms_scale(resid, ffn_gain).astype(jnp.bfloat16)
    flat = routes.reshape(N_EP, SEQS_DEV * TOP_K)
    onehot = (flat[..., None] == jnp.arange(EXPERTS, dtype=jnp.int32)[None, None, :]).astype(jnp.int32)
    before = jnp.cumsum(onehot, axis=1) - onehot
    slot = lax.optimization_barrier(jnp.sum(before * onehot, axis=-1)).astype(jnp.int32)
    block_ids = jnp.broadcast_to(jnp.arange(N_EP, dtype=jnp.int32)[:, None], flat.shape)
    row_of = (jnp.arange(SEQS_DEV * TOP_K, dtype=jnp.int32) // TOP_K)[None, :] + SEQS_DEV * block_ids
    table = jnp.zeros((EXPERTS, N_EP, CAP), jnp.int32).at[flat, block_ids, slot].set(row_of.astype(jnp.int32))
    piece = FF_EXP // N_TP

    def run_expert(args):
        w_gate, w_up, w_down, picks = args
        rows = moe_in[picks.reshape(-1)]
        gate = jnp.dot(rows, w_gate, preferred_element_type=jnp.float32)
        up = jnp.dot(rows, w_up, preferred_element_type=jnp.float32)
        hidden = (jax.nn.silu(gate) * up).astype(jnp.bfloat16)
        total = jnp.zeros((rows.shape[0], D), jnp.float32)
        for part in range(N_TP):
            term = jnp.dot(hidden[:, part * piece:(part + 1) * piece], w_down[part * piece:(part + 1) * piece], preferred_element_type=jnp.float32)
            total = total + term.astype(jnp.bfloat16).astype(jnp.float32)
        return total.astype(jnp.bfloat16).reshape(N_EP, CAP, D)
    results = lax.map(run_expert, (expert_gate, expert_up, expert_down, table))
    per_route = results[flat, block_ids, slot].astype(jnp.float32).reshape(SEQS, TOP_K, D)
    combined = lax.optimization_barrier(jnp.sum(per_route * route_weight[..., None], axis=1))
    layer_out = (resid + combined).astype(jnp.bfloat16)
    return (layer_out, new_state)
```

```python
import functools

import jax
import jax.numpy as jnp
from jax import lax
from jax.experimental import pallas as pl
from jax.experimental.pallas import tpu as pltpu
from jax.sharding import PartitionSpec as P

EPS = 1e-06
F32 = jnp.float32
BF16 = jnp.bfloat16
MESH = pl.DeviceIdType.MESH
LANES = 128


def rms_scale(rows, gain):
    return rows * lax.rsqrt(jnp.mean(rows * rows, axis=-1, keepdims=True) + EPS) * gain


def unit_rows(rows):
    return rows * lax.rsqrt(jnp.sum(rows * rows, axis=-1, keepdims=True) + EPS)


def silu(x):
    return x * (1.0 / (1.0 + jnp.exp(-x)))


def softplus(x):
    return jnp.maximum(x, 0.0) + jnp.log(1.0 + jnp.exp(-jnp.abs(x)))


def mixer_kernel(
    tok_h, gain_h, wq_h, wk_h, wv_h, wz_h, wd_h, wb_h, rate_h, bias_h, st_h, og_h, rt_h,
    ns_h, ho_ref, tab_ref,
    tok, gain, wbuf, wd, wb, rate, bias, st, og, rt, pq, wr, sem_small, sem_w, sem_s, sem_o,
):
    seqs = tok.shape[0]
    heads = st.shape[0]
    hd = st.shape[2]
    experts = 64

    small = [
        pltpu.make_async_copy(a, b, sem_small.at[i])
        for i, (a, b) in enumerate(
            [(tok_h, tok), (gain_h, gain), (wd_h, wd), (wb_h, wb), (rate_h, rate), (bias_h, bias), (og_h, og), (rt_h, rt)]
        )
    ]
    for c in small:
        c.start()
    w_in, s_in = [], []
    for h in range(heads):
        cols = pl.ds(h * hd, hd)
        w_in.append(
            [
                pltpu.make_async_copy(w.at[:, cols], wbuf.at[h, :, pl.ds(i * hd, hd)], sem_w.at[h, i])
                for i, w in enumerate((wq_h, wk_h, wv_h, wz_h))
            ]
        )
        s_in.append(pltpu.make_async_copy(st_h.at[:, h], st.at[h], sem_s.at[h]))
        for c in w_in[h]:
            c.start()
        s_in[h].start()
    for c in small:
        c.wait()

    ids = lax.broadcasted_iota(jnp.int32, (experts, seqs), 0)
    row = lax.broadcasted_iota(jnp.int32, (experts, seqs), 1)
    r = rt[...]
    hits = [ids == r[j : j + 1, :] for j in range(2)]
    either = hits[0] | hits[1]
    first = jnp.min(jnp.where(either, row, seqs), axis=1, keepdims=True)
    last = jnp.max(jnp.where(either, row, 0), axis=1, keepdims=True)
    first_row = jnp.where(first == seqs, 0, first)
    diag = lax.broadcasted_iota(jnp.int32, (experts, experts), 0) == lax.broadcasted_iota(
        jnp.int32, (experts, experts), 1
    )
    tab_ref[0:1, 0:experts] = jnp.sum(jnp.where(diag, first_row, 0), axis=0, keepdims=True)
    tab_ref[1:2, 0:experts] = jnp.sum(jnp.where(diag, last, 0), axis=0, keepdims=True)
    later = jnp.where(row > first, 1, 0)
    for j in range(2):
        slot = jnp.sum(jnp.where(hits[j], later, 0), axis=0, keepdims=True)
        tab_ref[2 + j : 3 + j, 0:seqs] = r[j : j + 1, :] * 2 + slot

    x = tok[...].astype(F32)
    normed = rms_scale(x, gain[...]).astype(BF16)
    normed32 = normed.astype(F32)

    def narrow(w, h):
        got = jnp.sum(normed32 * w[h : h + 1, :].astype(F32), axis=1, keepdims=True)
        return got.astype(BF16).astype(F32)

    fades, betas = [], []
    for h in range(heads):
        fade = jnp.exp(-rate[h] * softplus(narrow(wd, h) + bias[h]))
        fades.append(jnp.broadcast_to(fade, (seqs, hd)))
        betas.append(jnp.broadcast_to(1.0 / (1.0 + jnp.exp(-narrow(wb, h))), (seqs, hd)))

    out = []
    for h in range(heads):
        for c in w_in[h]:
            c.wait()
        raw = jnp.dot(normed, wbuf[h], preferred_element_type=F32).astype(BF16).astype(F32)
        q = unit_rows(silu(raw[:, 0:hd])) * hd ** (-0.5)
        k = unit_rows(silu(raw[:, hd : 2 * hd]))
        v = silu(raw[:, 2 * hd : 3 * hd])
        z = silu(raw[:, 3 * hd : 4 * hd])
        kq = jnp.sum(k * q, axis=1, keepdims=True)
        kt = k.T
        qt = q.T
        fade, beta = fades[h], betas[h]
        s_in[h].wait()
        for s in range(seqs):
            state = st[h, s]
            kcol = jnp.broadcast_to(kt[:, s : s + 1], (hd, hd))
            qcol = jnp.broadcast_to(qt[:, s : s + 1], (hd, hd))
            fade_s = fade[s : s + 1, :]
            pred = jnp.sum(state * kcol, axis=0, keepdims=True)
            pq[s : s + 1, :] = jnp.sum(state * qcol, axis=0, keepdims=True)
            written = beta[s : s + 1, :] * (v[s : s + 1, :] - fade_s * pred)
            wr[s : s + 1, :] = written
            st[h, s] = fade_s * state + kcol * written
            if s % 8 == 7:
                part = pl.ds(s - 7, 8)
                c = pltpu.make_async_copy(st.at[h, part], ns_h.at[part, h], sem_o.at[h, s // 8])
                c.start()
                out.append(c)
        read = fade * pq[...] + kq * wr[...]
        ho_ref[:, h * hd : (h + 1) * hd] = (rms_scale(read, og[...]) * z).astype(BF16)
    for c in out:
        c.wait()


def moe_kernel(
    n_ep, dims,
    ho_h, wo_h, tok_h, gain_h, eg_h, eu_h, ed_h, tab_ref, rw_ref,
    out_ref,
    ho, wo, tok, gain, wg, wu, wd, mix, mix_in, moe32, moe, send, recv, rows32, lhs, term32, rsend, ret, ret32, acc32, res,
    sem_l, sem_w, sem_x, sem_push, sem_pull, sem_send, sem_recv, sem_self, sem_back, sem_home, sem_bself,
):
    seqs, width = tok.shape
    half = width // 2
    tiles = width // LANES
    htiles = tiles // 2
    me = lax.axis_index("ep")
    core = lax.axis_index("tp")
    other = 1 - core
    par = lax.rem(me, 2)
    nz, ny, nx = dims

    loads = [
        pltpu.make_async_copy(a, b, sem_l.at[i])
        for i, (a, b) in enumerate([(ho_h, ho), (wo_h, wo), (tok_h, tok), (gain_h, gain)])
    ]
    for c in loads:
        c.start()
    wloads = [
        pltpu.make_async_copy(a, b.at[core], sem_w.at[i])
        for i, (a, b) in enumerate([(eg_h, wg), (eu_h, wu), (ed_h, wd)])
    ]
    for c in wloads:
        c.start()

    barrier = pltpu.get_barrier_semaphore()
    pl.semaphore_signal(barrier, inc=1, device_id={"ep": me, "tp": other}, device_id_type=MESH)

    def greet(j, _):
        d = lax.rem(me + j, n_ep)
        for t in range(2):
            pl.semaphore_signal(barrier, inc=1, device_id={"ep": d, "tp": t}, device_id_type=MESH)
        return 0

    lax.fori_loop(1, n_ep, greet, 0)

    loads[0].wait()
    loads[1].wait()
    mix[...] = jnp.dot(ho[...], wo[...], preferred_element_type=F32).astype(BF16)
    for c in loads[2:]:
        c.wait()
    pl.semaphore_wait(barrier, 2 * n_ep - 1)

    partner = {"ep": me, "tp": other}
    xchg = pltpu.make_async_remote_copy(
        mix, mix_in, sem_x.at[0], sem_x.at[1], device_id=partner, device_id_type=MESH
    )
    xchg.start()
    pushes = [
        pltpu.make_async_remote_copy(
            b.at[core], b.at[core], sem_push.at[i], sem_pull.at[i], device_id=partner, device_id_type=MESH
        )
        for i, b in enumerate((wg, wu, wd))
    ]
    wloads[0].wait()
    pushes[0].start()
    xchg.wait()

    resid = tok[...].astype(F32) + (mix[...].astype(F32) + mix_in[...].astype(F32))
    moe_in = rms_scale(resid, gain[...])
    for t in range(tiles):
        moe32[pl.ds(t, seqs, stride=tiles), :] = moe_in[:, t * LANES : (t + 1) * LANES]

    @pl.when(core == 0)
    def _():
        res[...] = resid[:, :half]

    @pl.when(core == 1)
    def _():
        res[...] = resid[:, half:]

    for t in range(seqs):
        moe[t] = moe32[t * tiles : (t + 1) * tiles, :].astype(BF16)
    for d in range(n_ep):
        send[d] = moe[tab_ref[core, d]]

    z0, y0, x0 = me // (ny * nx), lax.rem(me // nx, ny), lax.rem(me, nx)
    zs = [lax.rem(z0 + i, nz) * (ny * nx) for i in range(nz)]
    ys = [lax.rem(y0 + i, ny) * nx for i in range(ny)]
    xs = [lax.rem(x0 + i, nx) for i in range(nx)]
    hop = lambda i, n: min(i, n - i)
    order = sorted(
        [(a, b, c) for a in range(nz) for b in range(ny) for c in range(nx) if a or b or c],
        key=lambda o: -(hop(o[0], nz) + hop(o[1], ny) + hop(o[2], nx)),
    )
    my_row = core * (n_ep // 2) + me // 2
    for a, b, c in order:
        d = zs[a] + ys[b] + xs[c]
        pltpu.make_async_remote_copy(
            send.at[d], recv.at[my_row], sem_send, sem_recv, device_id={"ep": d, "tp": par}, device_id_type=MESH
        ).start()

    self_copy = pltpu.make_async_copy(send.at[me], recv.at[my_row], sem_recv)
    self_push = pltpu.make_async_remote_copy(
        send.at[me], recv.at[my_row], sem_self, sem_recv, device_id=partner, device_id_type=MESH
    )

    @pl.when(par == core)
    def _():
        self_copy.start()

    @pl.when(par != core)
    def _():
        self_push.start()

    for i in (1, 2):
        wloads[i].wait()
        pushes[i].start()

    pltpu.make_async_copy(recv, recv, sem_recv).wait()
    for t in range(n_ep):
        rows32[t * tiles : (t + 1) * tiles, :] = recv[t].astype(F32)
    for t in range(tiles):
        lhs[:, t * LANES : (t + 1) * LANES] = rows32[pl.ds(t, n_ep, stride=tiles), :].astype(BF16)
    pushes[0].wait()
    pushes[1].wait()
    hid = []
    for p in range(2):
        g = jnp.dot(lhs[...], wg[p], preferred_element_type=F32)
        u = jnp.dot(lhs[...], wu[p], preferred_element_type=F32)
        hid.append((silu(g) * u).astype(BF16))
    pushes[2].wait()
    for t in range(tiles):
        cols = slice(t * LANES, (t + 1) * LANES)
        got = jnp.dot(hid[0], wd[0, :, cols], preferred_element_type=F32) + jnp.dot(
            hid[1], wd[1, :, cols], preferred_element_type=F32
        )
        term32[pl.ds(t, n_ep, stride=tiles), :] = got
    for i in range(n_ep // 2):
        for hh in range(2):
            for s in range(2):
                at = (s * (n_ep // 2) + i) * tiles + hh * htiles
                rsend[hh, i, s] = term32[at : at + htiles, :].astype(BF16)

    mine = pl.ds(2 * me, 2)
    for a, b, c in order:
        if c % 2:
            continue
        d = zs[a] + ys[b] + lax.rem(x0 + jnp.where(par == core, c, c + 1), nx)
        for hh in range(2):
            pltpu.make_async_remote_copy(
                rsend.at[hh, d // 2], ret.at[mine], sem_back, sem_home, device_id={"ep": d, "tp": hh}, device_id_type=MESH
            ).start()
    last = zs[0] + ys[0] + lax.rem(x0 + jnp.where(par == core, 0, 1), nx)
    far = {"ep": last, "tp": other}
    back_other = pltpu.make_async_remote_copy(
        rsend.at[other, last // 2], ret.at[mine], sem_bself.at[0], sem_home, device_id=far, device_id_type=MESH
    )
    back_other.start()
    back_local = pltpu.make_async_copy(rsend.at[core, last // 2], ret.at[mine], sem_home)
    back_near = pltpu.make_async_remote_copy(
        rsend.at[core, last // 2], ret.at[mine], sem_bself.at[1], sem_home,
        device_id={"ep": last, "tp": core}, device_id_type=MESH,
    )

    @pl.when(par == core)
    def _():
        back_local.start()

    @pl.when(par != core)
    def _():
        back_near.start()

    pltpu.make_async_copy(send.at[pl.ds(0, n_ep - 1)], send.at[pl.ds(0, n_ep - 1)], sem_send).wait()

    @pl.when(par != core)
    def _():
        self_push.wait_send()

    pltpu.make_async_copy(ret, ret, sem_home).wait()
    for t in range(2 * n_ep):
        ret32[t] = ret[t].astype(F32)
    for t in range(seqs):
        acc = None
        for j in range(2):
            one = ret32[tab_ref[2 + j, t]] * rw_ref[j, t]
            acc = one if acc is None else acc + one
        acc32[t * htiles : (t + 1) * htiles, :] = acc
    for t in range(htiles):
        cols = slice(t * LANES, (t + 1) * LANES)
        out_ref[:, cols] = (res[:, cols] + acc32[pl.ds(t, seqs, stride=htiles), :]).astype(BF16)

    pltpu.make_async_copy(
        rsend.at[:, pl.ds(0, n_ep // 2 - 1)], rsend.at[:, pl.ds(0, n_ep // 2 - 1)], sem_back
    ).wait()
    back_other.wait_send()

    @pl.when(par != core)
    def _():
        back_near.wait_send()


HBM = pl.BlockSpec(memory_space=pltpu.HBM)
ANY = pl.BlockSpec(memory_space=pl.ANY)
VMEM = pl.BlockSpec(memory_space=pltpu.VMEM)
SMEM = pl.BlockSpec(memory_space=pltpu.SMEM)


def per_device(
    dims,
    tokens, attn_gain, w_query, w_key, w_value, w_zgate, w_decay, w_beta, decay_rate, decay_bias,
    state, out_gain, w_out, ffn_gain, expert_gate, expert_up, expert_down, routes, route_weight,
):
    seqs, width = tokens.shape
    heads, hd = state.shape[1], state.shape[2]
    n_ep = lax.axis_size("ep")
    tiles = width // LANES
    hidden = expert_gate.shape[2]
    dma = pltpu.SemaphoreType.DMA

    new_state, heads_out, table = pl.pallas_call(
        mixer_kernel,
        name="mixer",
        out_shape=(
            jax.ShapeDtypeStruct(state.shape, F32),
            jax.ShapeDtypeStruct((seqs, heads * hd), BF16),
            jax.ShapeDtypeStruct((8, LANES), jnp.int32),
        ),
        in_specs=[HBM] * 13,
        out_specs=(ANY, VMEM, VMEM),
        scratch_shapes=[
            pltpu.VMEM((seqs, width), BF16),
            pltpu.VMEM((1, width), F32),
            pltpu.VMEM((heads, width, 4 * hd), BF16),
            pltpu.VMEM((heads, width), BF16),
            pltpu.VMEM((heads, width), BF16),
            pltpu.SMEM((heads,), F32),
            pltpu.SMEM((heads,), F32),
            pltpu.VMEM((heads, seqs, hd, hd), F32),
            pltpu.VMEM((1, hd), F32),
            pltpu.VMEM((2, seqs), jnp.int32),
            pltpu.VMEM((seqs, hd), F32),
            pltpu.VMEM((seqs, hd), F32),
            dma((8,)),
            dma((heads, 4)),
            dma((heads,)),
            dma((heads, seqs // 8)),
        ],
        compiler_params=pltpu.CompilerParams(vmem_limit_bytes=24 * 2**20),
        cost_estimate=pl.CostEstimate(flops=10**8, bytes_accessed=2 * 10**7, transcendentals=0),
    )(
        tokens, attn_gain.reshape(1, width), w_query, w_key, w_value, w_zgate, w_decay.T, w_beta.T,
        decay_rate, decay_bias, state, out_gain.reshape(1, hd), routes.T,
    )

    layer_out = pl.pallas_call(
        functools.partial(moe_kernel, n_ep, dims),
        name="experts",
        out_shape=jax.ShapeDtypeStruct((seqs, width // 2), BF16),
        in_specs=[ANY, HBM, ANY, ANY, HBM, HBM, HBM, SMEM, SMEM],
        out_specs=VMEM,
        scratch_shapes=[
            pltpu.VMEM((seqs, heads * hd), BF16),
            pltpu.VMEM(w_out.shape, BF16),
            pltpu.VMEM((seqs, width), BF16),
            pltpu.VMEM((1, width), F32),
            pltpu.VMEM((2, width, hidden), BF16),
            pltpu.VMEM((2, width, hidden), BF16),
            pltpu.VMEM((2, hidden, width), BF16),
            pltpu.VMEM((seqs, width), BF16),
            pltpu.VMEM((seqs, width), BF16),
            pltpu.VMEM((seqs * tiles, LANES), F32),
            pltpu.VMEM((seqs, tiles, LANES), BF16),
            pltpu.VMEM((n_ep, tiles, LANES), BF16),
            pltpu.VMEM((n_ep, tiles, LANES), BF16),
            pltpu.VMEM((n_ep * tiles, LANES), F32),
            pltpu.VMEM((n_ep, width), BF16),
            pltpu.VMEM((n_ep * tiles, LANES), F32),
            pltpu.VMEM((2, n_ep // 2, 2, tiles // 2, LANES), BF16),
            pltpu.VMEM((2 * n_ep, tiles // 2, LANES), BF16),
            pltpu.VMEM((2 * n_ep, tiles // 2, LANES), F32),
            pltpu.VMEM((seqs * tiles // 2, LANES), F32),
            pltpu.VMEM((seqs, width // 2), F32),
            dma((4,)),
            dma((3,)),
            dma((2,)),
            dma((3,)),
            dma((3,)),
            dma,
            dma,
            dma,
            dma,
            dma,
            dma((2,)),
        ],
        compiler_params=pltpu.CompilerParams(
            collective_id=0, has_side_effects=True, vmem_limit_bytes=24 * 2**20
        ),
        cost_estimate=pl.CostEstimate(flops=10**8, bytes_accessed=10**7, transcendentals=0),
    )(
        heads_out, w_out, tokens, ffn_gain.reshape(1, width), expert_gate[0], expert_up[0],
        expert_down[0], table, route_weight.T,
    )
    return (layer_out, new_state)


def solution(mesh):
    in_specs = (
        P("ep", None), P(), P(None, "tp"), P(None, "tp"), P(None, "tp"), P(None, "tp"), P(None, "tp"), P(None, "tp"),
        P("tp"), P("tp"), P("ep", "tp", None, None), P(), P("tp", None), P(), P("ep", None, "tp"), P("ep", None, "tp"),
        P("ep", "tp", None), P("ep", None), P("ep", None),
    )
    out_specs = (P("ep", "tp"), P("ep", "tp", None, None))
    side = round(mesh.shape["ep"] ** (1 / 3))
    dims = (side, side, side)
    return jax.shard_map(
        functools.partial(per_device, dims), mesh=mesh, in_specs=in_specs, out_specs=out_specs, check_vma=False
    )
```

```python
import functools

import jax
import jax.numpy as jnp
from jax import lax
from jax.experimental import pallas as pl
from jax.experimental.pallas import tpu as pltpu
from jax.sharding import PartitionSpec as P

EPS = 1e-06
F32 = jnp.float32
BF16 = jnp.bfloat16
MESH = pl.DeviceIdType.MESH
LANES = 128


def rms_scale(rows, gain):
    return rows * lax.rsqrt(jnp.mean(rows * rows, axis=-1, keepdims=True) + EPS) * gain


def unit_rows(rows):
    return rows * lax.rsqrt(jnp.sum(rows * rows, axis=-1, keepdims=True) + EPS)


def silu(x):
    return x * (1.0 / (1.0 + jnp.exp(-x)))


def softplus(x):
    return jnp.maximum(x, 0.0) + jnp.log(1.0 + jnp.exp(-jnp.abs(x)))


def mixer_kernel(
    tok_h, gain_h, wq_h, wk_h, wv_h, wz_h, wd_h, wb_h, rate_h, bias_h, st_h, og_h, rt_h,
    ns_h, ho_ref, tab_ref,
    tok, gain, wbuf, wd, wb, rate, bias, st, og, rt, pq, wr, sem_small, sem_w, sem_s, sem_o,
):
    seqs = tok.shape[0]
    heads = st.shape[0]
    hd = st.shape[2]
    experts = 64

    small = [
        pltpu.make_async_copy(a, b, sem_small.at[i])
        for i, (a, b) in enumerate(
            [(tok_h, tok), (gain_h, gain), (wd_h, wd), (wb_h, wb), (rate_h, rate), (bias_h, bias), (og_h, og), (rt_h, rt)]
        )
    ]
    for c in small:
        c.start()
    w_in, s_in = [], []
    for h in range(heads):
        cols = pl.ds(h * hd, hd)
        w_in.append(
            [
                pltpu.make_async_copy(w.at[:, cols], wbuf.at[h, :, pl.ds(i * hd, hd)], sem_w.at[h, i])
                for i, w in enumerate((wq_h, wk_h, wv_h, wz_h))
            ]
        )
        s_in.append(pltpu.make_async_copy(st_h.at[:, h], st.at[h], sem_s.at[h]))
        for c in w_in[h]:
            c.start()
        s_in[h].start()
    for c in small:
        c.wait()

    ids = lax.broadcasted_iota(jnp.int32, (experts, seqs), 0)
    row = lax.broadcasted_iota(jnp.int32, (experts, seqs), 1)
    r = rt[...]
    hits = [ids == r[j : j + 1, :] for j in range(2)]
    either = hits[0] | hits[1]
    first = jnp.min(jnp.where(either, row, seqs), axis=1, keepdims=True)
    last = jnp.max(jnp.where(either, row, 0), axis=1, keepdims=True)
    first_row = jnp.where(first == seqs, 0, first)
    diag = lax.broadcasted_iota(jnp.int32, (experts, experts), 0) == lax.broadcasted_iota(
        jnp.int32, (experts, experts), 1
    )
    tab_ref[0:1, 0:experts] = jnp.sum(jnp.where(diag, first_row, 0), axis=0, keepdims=True)
    tab_ref[1:2, 0:experts] = jnp.sum(jnp.where(diag, last, 0), axis=0, keepdims=True)
    later = jnp.where(row > first, 1, 0)
    for j in range(2):
        slot = jnp.sum(jnp.where(hits[j], later, 0), axis=0, keepdims=True)
        tab_ref[2 + j : 3 + j, 0:seqs] = r[j : j + 1, :] * 2 + slot

    x = tok[...].astype(F32)
    normed = rms_scale(x, gain[...]).astype(BF16)
    normed32 = normed.astype(F32)

    def narrow(w, h):
        got = jnp.sum(normed32 * w[h : h + 1, :].astype(F32), axis=1, keepdims=True)
        return got.astype(BF16).astype(F32)

    fades, betas = [], []
    for h in range(heads):
        fade = jnp.exp(-rate[h] * softplus(narrow(wd, h) + bias[h]))
        fades.append(jnp.broadcast_to(fade, (seqs, hd)))
        betas.append(jnp.broadcast_to(1.0 / (1.0 + jnp.exp(-narrow(wb, h))), (seqs, hd)))

    out = []
    for h in range(heads):
        for c in w_in[h]:
            c.wait()
        raw = jnp.dot(normed, wbuf[h], preferred_element_type=F32).astype(BF16).astype(F32)
        q = unit_rows(silu(raw[:, 0:hd])) * hd ** (-0.5)
        k = unit_rows(silu(raw[:, hd : 2 * hd]))
        v = silu(raw[:, 2 * hd : 3 * hd])
        z = silu(raw[:, 3 * hd : 4 * hd])
        kq = jnp.sum(k * q, axis=1, keepdims=True)
        kt = k.T
        qt = q.T
        fade, beta = fades[h], betas[h]
        s_in[h].wait()
        for s in range(seqs):
            state = st[h, s]
            kcol = jnp.broadcast_to(kt[:, s : s + 1], (hd, hd))
            qcol = jnp.broadcast_to(qt[:, s : s + 1], (hd, hd))
            fade_s = fade[s : s + 1, :]
            pred = jnp.sum(state * kcol, axis=0, keepdims=True)
            pq[s : s + 1, :] = jnp.sum(state * qcol, axis=0, keepdims=True)
            written = beta[s : s + 1, :] * (v[s : s + 1, :] - fade_s * pred)
            wr[s : s + 1, :] = written
            st[h, s] = fade_s * state + kcol * written
            if s % 8 == 7:
                part = pl.ds(s - 7, 8)
                c = pltpu.make_async_copy(st.at[h, part], ns_h.at[part, h], sem_o.at[h, s // 8])
                c.start()
                out.append(c)
        read = fade * pq[...] + kq * wr[...]
        ho_ref[:, h * hd : (h + 1) * hd] = (rms_scale(read, og[...]) * z).astype(BF16)
    for c in out:
        c.wait()


def moe_kernel(
    n_ep, dims,
    ho_h, wo_h, tok_h, gain_h, eg_h, eu_h, ed_h, tab_ref, rw_ref,
    out_ref,
    ho, wo, tok, gain, wg, wu, wd, mix, mix_in, moe32, moe, send, recv, rows32, lhs, term32, rsend, ret, ret32, acc32, res,
    sem_l, sem_w, sem_x, sem_push, sem_pull, sem_send, sem_recv, sem_self, sem_back, sem_home, sem_bself,
):
    seqs, width = tok.shape
    half = width // 2
    tiles = width // LANES
    htiles = tiles // 2
    me = lax.axis_index("ep")
    core = lax.axis_index("tp")
    other = 1 - core
    par = lax.rem(me, 2)
    nz, ny, nx = dims

    loads = [
        pltpu.make_async_copy(a, b, sem_l.at[i])
        for i, (a, b) in enumerate([(ho_h, ho), (wo_h, wo), (tok_h, tok), (gain_h, gain)])
    ]
    for c in loads:
        c.start()
    wloads = [
        pltpu.make_async_copy(a, b.at[core], sem_w.at[i])
        for i, (a, b) in enumerate([(eg_h, wg), (eu_h, wu), (ed_h, wd)])
    ]
    for c in wloads:
        c.start()

    barrier = pltpu.get_barrier_semaphore()
    pl.semaphore_signal(barrier, inc=1, device_id={"ep": me, "tp": other}, device_id_type=MESH)

    def greet(j, _):
        d = lax.rem(me + j, n_ep)
        for t in range(2):
            pl.semaphore_signal(barrier, inc=1, device_id={"ep": d, "tp": t}, device_id_type=MESH)
        return 0

    lax.fori_loop(1, n_ep, greet, 0)

    loads[0].wait()
    loads[1].wait()
    mix[...] = jnp.dot(ho[...], wo[...], preferred_element_type=F32).astype(BF16)
    for c in loads[2:]:
        c.wait()
    pl.semaphore_wait(barrier, 2 * n_ep - 1)

    partner = {"ep": me, "tp": other}
    xchg = pltpu.make_async_remote_copy(
        mix, mix_in, sem_x.at[0], sem_x.at[1], device_id=partner, device_id_type=MESH
    )
    xchg.start()
    pushes = [
        pltpu.make_async_remote_copy(
            b.at[core], b.at[core], sem_push.at[i], sem_pull.at[i], device_id=partner, device_id_type=MESH
        )
        for i, b in enumerate((wg, wu, wd))
    ]
    wloads[0].wait()
    pushes[0].start()
    xchg.wait()

    resid = tok[...].astype(F32) + (mix[...].astype(F32) + mix_in[...].astype(F32))
    moe_in = rms_scale(resid, gain[...])
    for t in range(tiles):
        moe32[pl.ds(t, seqs, stride=tiles), :] = moe_in[:, t * LANES : (t + 1) * LANES]

    @pl.when(core == 0)
    def _():
        res[...] = resid[:, :half]

    @pl.when(core == 1)
    def _():
        res[...] = resid[:, half:]

    for t in range(seqs):
        moe[t] = moe32[t * tiles : (t + 1) * tiles, :].astype(BF16)
    for d in range(n_ep):
        send[d] = moe[tab_ref[core, d]]

    z0, y0, x0 = me // (ny * nx), lax.rem(me // nx, ny), lax.rem(me, nx)
    zs = [lax.rem(z0 + i, nz) * (ny * nx) for i in range(nz)]
    ys = [lax.rem(y0 + i, ny) * nx for i in range(ny)]
    xs = [lax.rem(x0 + i, nx) for i in range(nx)]
    hop = lambda i, n: min(i, n - i)
    order = sorted(
        [(a, b, c) for a in range(nz) for b in range(ny) for c in range(nx) if a or b or c],
        key=lambda o: -(hop(o[0], nz) + hop(o[1], ny) + hop(o[2], nx)),
    )
    my_row = core * (n_ep // 2) + me // 2
    for a, b, c in order:
        d = zs[a] + ys[b] + xs[c]
        pltpu.make_async_remote_copy(
            send.at[d], recv.at[my_row], sem_send, sem_recv, device_id={"ep": d, "tp": par}, device_id_type=MESH
        ).start()

    self_copy = pltpu.make_async_copy(send.at[me], recv.at[my_row], sem_recv)
    self_push = pltpu.make_async_remote_copy(
        send.at[me], recv.at[my_row], sem_self, sem_recv, device_id=partner, device_id_type=MESH
    )

    @pl.when(par == core)
    def _():
        self_copy.start()

    @pl.when(par != core)
    def _():
        self_push.start()

    for i in (1, 2):
        wloads[i].wait()
        pushes[i].start()

    pltpu.make_async_copy(recv, recv, sem_recv).wait()
    for t in range(n_ep):
        rows32[t * tiles : (t + 1) * tiles, :] = recv[t].astype(F32)
    for t in range(tiles):
        lhs[:, t * LANES : (t + 1) * LANES] = rows32[pl.ds(t, n_ep, stride=tiles), :].astype(BF16)
    pushes[0].wait()
    pushes[1].wait()
    hid = []
    for p in range(2):
        g = jnp.dot(lhs[...], wg[p], preferred_element_type=F32)
        u = jnp.dot(lhs[...], wu[p], preferred_element_type=F32)
        hid.append((silu(g) * u).astype(BF16))
    pushes[2].wait()
    for t in range(tiles):
        cols = slice(t * LANES, (t + 1) * LANES)
        got = jnp.dot(hid[0], wd[0, :, cols], preferred_element_type=F32) + jnp.dot(
            hid[1], wd[1, :, cols], preferred_element_type=F32
        )
        term32[pl.ds(t, n_ep, stride=tiles), :] = got
    for i in range(n_ep // 2):
        for hh in range(2):
            for s in range(2):
                at = (s * (n_ep // 2) + i) * tiles + hh * htiles
                rsend[hh, i, s] = term32[at : at + htiles, :].astype(BF16)

    mine = pl.ds(2 * me, 2)
    for a, b, c in order:
        if c % 2:
            continue
        d = zs[a] + ys[b] + lax.rem(x0 + jnp.where(par == core, c, c + 1), nx)
        for hh in range(2):
            pltpu.make_async_remote_copy(
                rsend.at[hh, d // 2], ret.at[mine], sem_back, sem_home, device_id={"ep": d, "tp": hh}, device_id_type=MESH
            ).start()
    last = zs[0] + ys[0] + lax.rem(x0 + jnp.where(par == core, 0, 1), nx)
    far = {"ep": last, "tp": other}
    back_other = pltpu.make_async_remote_copy(
        rsend.at[other, last // 2], ret.at[mine], sem_bself.at[0], sem_home, device_id=far, device_id_type=MESH
    )
    back_other.start()
    back_local = pltpu.make_async_copy(rsend.at[core, last // 2], ret.at[mine], sem_home)
    back_near = pltpu.make_async_remote_copy(
        rsend.at[core, last // 2], ret.at[mine], sem_bself.at[1], sem_home,
        device_id={"ep": last, "tp": core}, device_id_type=MESH,
    )

    @pl.when(par == core)
    def _():
        back_local.start()

    @pl.when(par != core)
    def _():
        back_near.start()

    pltpu.make_async_copy(send.at[pl.ds(0, n_ep - 1)], send.at[pl.ds(0, n_ep - 1)], sem_send).wait()

    @pl.when(par != core)
    def _():
        self_push.wait_send()

    pltpu.make_async_copy(ret, ret, sem_home).wait()
    for t in range(2 * n_ep):
        ret32[t] = ret[t].astype(F32)
    for t in range(seqs):
        acc = None
        for j in range(2):
            one = ret32[tab_ref[2 + j, t]] * rw_ref[j, t]
            acc = one if acc is None else acc + one
        acc32[t * htiles : (t + 1) * htiles, :] = acc
    for t in range(htiles):
        cols = slice(t * LANES, (t + 1) * LANES)
        out_ref[:, cols] = (res[:, cols] + acc32[pl.ds(t, seqs, stride=htiles), :]).astype(BF16)

    pltpu.make_async_copy(
        rsend.at[:, pl.ds(0, n_ep // 2 - 1)], rsend.at[:, pl.ds(0, n_ep // 2 - 1)], sem_back
    ).wait()
    back_other.wait_send()

    @pl.when(par != core)
    def _():
        back_near.wait_send()


HBM = pl.BlockSpec(memory_space=pltpu.HBM)
ANY = pl.BlockSpec(memory_space=pl.ANY)
VMEM = pl.BlockSpec(memory_space=pltpu.VMEM)
SMEM = pl.BlockSpec(memory_space=pltpu.SMEM)


def keep(a):
    return pltpu.with_memory_space_constraint(a, pltpu.HBM)


def per_device(
    dims,
    tokens, attn_gain, w_query, w_key, w_value, w_zgate, w_decay, w_beta, decay_rate, decay_bias,
    state, out_gain, w_out, ffn_gain, expert_gate, expert_up, expert_down, routes, route_weight,
):
    seqs, width = tokens.shape
    heads, hd = state.shape[1], state.shape[2]
    n_ep = lax.axis_size("ep")
    tiles = width // LANES
    hidden = expert_gate.shape[2]
    dma = pltpu.SemaphoreType.DMA

    new_state, heads_out, table = pl.pallas_call(
        mixer_kernel,
        name="mixer",
        out_shape=(
            jax.ShapeDtypeStruct(state.shape, F32),
            jax.ShapeDtypeStruct((seqs, heads * hd), BF16),
            jax.ShapeDtypeStruct((8, LANES), jnp.int32),
        ),
        in_specs=[HBM] * 13,
        out_specs=(ANY, VMEM, VMEM),
        scratch_shapes=[
            pltpu.VMEM((seqs, width), BF16),
            pltpu.VMEM((1, width), F32),
            pltpu.VMEM((heads, width, 4 * hd), BF16),
            pltpu.VMEM((heads, width), BF16),
            pltpu.VMEM((heads, width), BF16),
            pltpu.SMEM((heads,), F32),
            pltpu.SMEM((heads,), F32),
            pltpu.VMEM((heads, seqs, hd, hd), F32),
            pltpu.VMEM((1, hd), F32),
            pltpu.VMEM((2, seqs), jnp.int32),
            pltpu.VMEM((seqs, hd), F32),
            pltpu.VMEM((seqs, hd), F32),
            dma((8,)),
            dma((heads, 4)),
            dma((heads,)),
            dma((heads, seqs // 8)),
        ],
        compiler_params=pltpu.CompilerParams(vmem_limit_bytes=24 * 2**20),
        cost_estimate=pl.CostEstimate(flops=10**8, bytes_accessed=2 * 10**7, transcendentals=0),
    )(
        *[
            keep(a)
            for a in (
                tokens, attn_gain.reshape(1, width), w_query, w_key, w_value, w_zgate, w_decay.T, w_beta.T,
                decay_rate, decay_bias, state, out_gain.reshape(1, hd), routes.T,
            )
        ]
    )

    layer_out = pl.pallas_call(
        functools.partial(moe_kernel, n_ep, dims),
        name="experts",
        out_shape=jax.ShapeDtypeStruct((seqs, width // 2), BF16),
        in_specs=[ANY, HBM, ANY, ANY, HBM, HBM, HBM, SMEM, SMEM],
        out_specs=VMEM,
        scratch_shapes=[
            pltpu.VMEM((seqs, heads * hd), BF16),
            pltpu.VMEM(w_out.shape, BF16),
            pltpu.VMEM((seqs, width), BF16),
            pltpu.VMEM((1, width), F32),
            pltpu.VMEM((2, width, hidden), BF16),
            pltpu.VMEM((2, width, hidden), BF16),
            pltpu.VMEM((2, hidden, width), BF16),
            pltpu.VMEM((seqs, width), BF16),
            pltpu.VMEM((seqs, width), BF16),
            pltpu.VMEM((seqs * tiles, LANES), F32),
            pltpu.VMEM((seqs, tiles, LANES), BF16),
            pltpu.VMEM((n_ep, tiles, LANES), BF16),
            pltpu.VMEM((n_ep, tiles, LANES), BF16),
            pltpu.VMEM((n_ep * tiles, LANES), F32),
            pltpu.VMEM((n_ep, width), BF16),
            pltpu.VMEM((n_ep * tiles, LANES), F32),
            pltpu.VMEM((2, n_ep // 2, 2, tiles // 2, LANES), BF16),
            pltpu.VMEM((2 * n_ep, tiles // 2, LANES), BF16),
            pltpu.VMEM((2 * n_ep, tiles // 2, LANES), F32),
            pltpu.VMEM((seqs * tiles // 2, LANES), F32),
            pltpu.VMEM((seqs, width // 2), F32),
            dma((4,)),
            dma((3,)),
            dma((2,)),
            dma((3,)),
            dma((3,)),
            dma,
            dma,
            dma,
            dma,
            dma,
            dma((2,)),
        ],
        compiler_params=pltpu.CompilerParams(
            collective_id=0, has_side_effects=True, vmem_limit_bytes=24 * 2**20
        ),
        cost_estimate=pl.CostEstimate(flops=10**8, bytes_accessed=10**7, transcendentals=0),
    )(
        heads_out, keep(w_out), keep(tokens), ffn_gain.reshape(1, width), keep(expert_gate[0]), keep(expert_up[0]),
        keep(expert_down[0]), table, route_weight.T,
    )
    return (layer_out, new_state)


def solution(mesh):
    in_specs = (
        P("ep", None), P(), P(None, "tp"), P(None, "tp"), P(None, "tp"), P(None, "tp"), P(None, "tp"), P(None, "tp"),
        P("tp"), P("tp"), P("ep", "tp", None, None), P(), P("tp", None), P(), P("ep", None, "tp"), P("ep", None, "tp"),
        P("ep", "tp", None), P("ep", None), P("ep", None),
    )
    out_specs = (P("ep", "tp"), P("ep", "tp", None, None))
    side = round(mesh.shape["ep"] ** (1 / 3))
    dims = (side, side, side)
    return jax.shard_map(
        functools.partial(per_device, dims), mesh=mesh, in_specs=in_specs, out_specs=out_specs, check_vma=False
    )
```

```python
import functools

import jax
import jax.numpy as jnp
from jax import lax
from jax.experimental import pallas as pl
from jax.experimental.pallas import tpu as pltpu
from jax.sharding import PartitionSpec as P

EPS = 1e-06
F32 = jnp.float32
BF16 = jnp.bfloat16
MESH = pl.DeviceIdType.MESH
LANES = 128


def rms_scale(rows, gain):
    return rows * lax.rsqrt(jnp.mean(rows * rows, axis=-1, keepdims=True) + EPS) * gain


def unit_rows(rows):
    return rows * lax.rsqrt(jnp.sum(rows * rows, axis=-1, keepdims=True) + EPS)


def silu(x):
    return x * (1.0 / (1.0 + jnp.exp(-x)))


def softplus(x):
    return jnp.maximum(x, 0.0) + jnp.log(1.0 + jnp.exp(-jnp.abs(x)))


def layer_kernel(
    n_ep, dims,
    tok_h, gain_h, wq_h, wk_h, wv_h, wz_h, wd_h, wb_h, rate_h, bias_h, st_h, og_h, wo_h, fgain_h, eg_h, eu_h, ed_h, rt_h, rw_h,
    out_ref, ns_ref,
    tok, gain, wbuf, wd, wb, rate, bias, og, wo, fgain, rt, rw, tab_v, tab,
    kts, written, fades, ho,
    wg, wu, wdn, mix, mix_in, moe32, moe, send, recv, rows32, lhs, term32, rsend, ret, ret32, acc32, res,
    sem_small, sem_w, sem_s, sem_wo, sem_tab, sem_e, sem_x, sem_push, sem_pull, sem_send, sem_recv, sem_self, sem_back, sem_home, sem_bself,
):
    seqs, width = tok.shape
    heads, hd = kts.shape[0], kts.shape[1]
    half = width // 2
    tiles = width // LANES
    htiles = tiles // 2
    me = lax.axis_index("ep")
    core = lax.axis_index("tp")
    other = 1 - core
    par = lax.rem(me, 2)
    shift = jnp.where(par == core, 0, 1)
    nz, ny, nx = dims

    small = [
        pltpu.make_async_copy(a, b, sem_small.at[i])
        for i, (a, b) in enumerate(
            [
                (tok_h, tok), (gain_h, gain), (wd_h, wd), (wb_h, wb), (rate_h, rate), (bias_h, bias), (og_h, og),
                (rt_h, rt), (fgain_h, fgain), (rw_h, rw),
            ]
        )
    ]
    for c in small:
        c.start()
    big = []
    for h in range(heads):
        cols = pl.ds(h * hd, hd)
        big.append(
            [
                pltpu.make_async_copy(w.at[:, cols], wbuf.at[h, :, pl.ds(i * hd, hd)], sem_w.at[h, i])
                for i, w in enumerate((wq_h, wk_h, wv_h, wz_h))
            ]
            + [pltpu.make_async_copy(st_h.at[:, h], ns_ref.at[:, h], sem_s.at[h])]
        )
    wo_in = pltpu.make_async_copy(wo_h, wo, sem_wo)
    e_in = [
        pltpu.make_async_copy(a, b.at[core], sem_e.at[i])
        for i, (a, b) in enumerate([(eg_h, wg), (eu_h, wu), (ed_h, wdn)])
    ]
    for c in big[0]:
        c.start()

    z0, y0, x0 = me // (ny * nx), lax.rem(me // nx, ny), lax.rem(me, nx)
    zs = [lax.rem(z0 + i, nz) * (ny * nx) for i in range(nz)]
    ys = [lax.rem(y0 + i, ny) * nx for i in range(ny)]
    xs = [lax.rem(x0 + i, nx) for i in range(nx)]
    xp = [lax.rem(x0 + i + shift, nx) for i in range(nx)]
    hop = lambda i, n: min(i, n - i)
    order = sorted(
        [(a, b, c) for a in range(nz) for b in range(ny) for c in range(nx)],
        key=lambda o: -(hop(o[0], nz) + hop(o[1], ny) + hop(o[2], nx)),
    )
    partner = {"ep": me, "tp": other}

    barrier = pltpu.get_barrier_semaphore()
    for a, b, c in order[:-1]:
        pl.semaphore_signal(
            barrier, inc=1, device_id={"ep": zs[a] + ys[b] + xs[c], "tp": par}, device_id_type=MESH
        )
        if c % 2 == 0:
            pl.semaphore_signal(
                barrier, inc=1, device_id={"ep": zs[a] + ys[b] + xp[c], "tp": 1 - par}, device_id_type=MESH
            )

    @pl.when(par != core)
    def _():
        pl.semaphore_signal(
            barrier, inc=1, device_id={"ep": zs[0] + ys[0] + xp[0], "tp": 1 - par}, device_id_type=MESH
        )

    pl.semaphore_signal(barrier, inc=1, device_id=partner, device_id_type=MESH)

    for c in small:
        c.wait()
    for c in big[1]:
        c.start()

    ids = lax.broadcasted_iota(jnp.int32, (n_ep, seqs), 0)
    row = lax.broadcasted_iota(jnp.int32, (n_ep, seqs), 1)
    r = rt[...]
    hits = [ids == r[j : j + 1, :] for j in range(2)]
    either = hits[0] | hits[1]
    first = jnp.min(jnp.where(either, row, seqs), axis=1, keepdims=True)
    last = jnp.max(jnp.where(either, row, 0), axis=1, keepdims=True)
    first_row = jnp.where(first == seqs, 0, first)
    diag = lax.broadcasted_iota(jnp.int32, (n_ep, n_ep), 0) == lax.broadcasted_iota(jnp.int32, (n_ep, n_ep), 1)
    tab_v[0:1, 0:n_ep] = jnp.sum(jnp.where(diag, first_row, 0), axis=0, keepdims=True)
    tab_v[1:2, 0:n_ep] = jnp.sum(jnp.where(diag, last, 0), axis=0, keepdims=True)
    later = jnp.where(row > first, 1, 0)
    for j in range(2):
        slot = jnp.sum(jnp.where(hits[j], later, 0), axis=0, keepdims=True)
        tab_v[2 + j : 3 + j, 0:seqs] = r[j : j + 1, :] * 2 + slot

    x = tok[...].astype(F32)
    normed = rms_scale(x, gain[...]).astype(BF16)
    normed32 = normed.astype(F32)

    def narrow(w, h):
        got = jnp.sum(normed32 * w[h : h + 1, :].astype(F32), axis=1, keepdims=True)
        return got.astype(BF16).astype(F32)

    betas = []
    for h in range(heads):
        fade = jnp.exp(-rate[h] * softplus(narrow(wd, h) + bias[h]))
        fades[h] = jnp.broadcast_to(fade, (seqs, hd))
        betas.append(jnp.broadcast_to(1.0 / (1.0 + jnp.exp(-narrow(wb, h))), (seqs, hd)))

    tab_copy = pltpu.make_async_copy(tab_v, tab, sem_tab)
    tab_copy.start()

    sub = lax.broadcasted_iota(jnp.int32, (8, hd), 0)
    for h in range(heads):
        for c in big[h]:
            c.wait()
        if h + 2 < heads:
            for c in big[h + 2]:
                c.start()
        if h + 2 == heads:
            wo_in.start()
        if h + 1 == heads:
            for c in e_in:
                c.start()
        raw = jnp.dot(normed, wbuf[h], preferred_element_type=F32).astype(BF16).astype(F32)
        q = unit_rows(silu(raw[:, 0:hd])) * hd ** (-0.5)
        k = unit_rows(silu(raw[:, hd : 2 * hd]))
        v = silu(raw[:, 2 * hd : 3 * hd])
        z = silu(raw[:, 3 * hd : 4 * hd])
        kq = jnp.sum(k * q, axis=1, keepdims=True)
        kts[h] = k.T
        preds, sqs = [], []
        for g in range(seqs // 8):
            pair = jnp.concatenate([k[g * 8 : g * 8 + 8], q[g * 8 : g * 8 + 8]], axis=0).astype(BF16)
            pred = sq = None
            for s in range(0, 8, 2):
                both = jnp.concatenate([ns_ref[g * 8 + s, h], ns_ref[g * 8 + s + 1, h]], axis=1).astype(BF16)
                got = jnp.dot(pair, both, preferred_element_type=F32)
                for i in range(2):
                    one, two = got[0:8, i * hd : (i + 1) * hd], got[8:16, i * hd : (i + 1) * hd]
                    pred = one if pred is None else jnp.where(sub == s + i, one, pred)
                    sq = two if sq is None else jnp.where(sub == s + i, two, sq)
            preds.append(pred)
            sqs.append(sq)
        pred, sq = jnp.concatenate(preds, axis=0), jnp.concatenate(sqs, axis=0)
        fade = fades[h]
        wr = betas[h] * (v - fade * pred)
        written[h] = wr
        read = fade * sq + kq * wr
        ho[:, h * hd : (h + 1) * hd] = (rms_scale(read, og[...]) * z).astype(BF16)

    wo_in.wait()
    mix[...] = jnp.dot(ho[...], wo[...], preferred_element_type=F32).astype(BF16)
    pl.semaphore_wait(barrier, 95 + shift)

    xchg = pltpu.make_async_remote_copy(
        mix, mix_in, sem_x.at[0], sem_x.at[1], device_id=partner, device_id_type=MESH
    )
    xchg.start()
    pushes = [
        pltpu.make_async_remote_copy(
            b.at[core], b.at[core], sem_push.at[i], sem_pull.at[i], device_id=partner, device_id_type=MESH
        )
        for i, b in enumerate((wg, wu, wdn))
    ]
    e_in[0].wait()
    pushes[0].start()
    tab_copy.wait()
    xchg.wait()

    resid = tok[...].astype(F32) + (mix[...].astype(F32) + mix_in[...].astype(F32))
    moe_in = rms_scale(resid, fgain[...])
    for t in range(tiles):
        moe32[pl.ds(t, seqs, stride=tiles), :] = moe_in[:, t * LANES : (t + 1) * LANES]

    @pl.when(core == 0)
    def _():
        res[...] = resid[:, :half]

    @pl.when(core == 1)
    def _():
        res[...] = resid[:, half:]

    for t in range(seqs):
        moe[t] = moe32[t * tiles : (t + 1) * tiles, :].astype(BF16)
    for d in range(n_ep):
        send[d] = moe[tab[core, d]]

    my_row = core * (n_ep // 2) + me // 2
    for a, b, c in order[:-1]:
        d = zs[a] + ys[b] + xs[c]
        pltpu.make_async_remote_copy(
            send.at[d], recv.at[my_row], sem_send, sem_recv, device_id={"ep": d, "tp": par}, device_id_type=MESH
        ).start()
    self_copy = pltpu.make_async_copy(send.at[me], recv.at[my_row], sem_recv)
    self_push = pltpu.make_async_remote_copy(
        send.at[me], recv.at[my_row], sem_self, sem_recv, device_id=partner, device_id_type=MESH
    )

    @pl.when(par == core)
    def _():
        self_copy.start()

    @pl.when(par != core)
    def _():
        self_push.start()

    for i in (1, 2):
        e_in[i].wait()
        pushes[i].start()

    for h in range(heads):
        for s in range(seqs):
            kcol = jnp.broadcast_to(kts[h, :, s : s + 1], (hd, hd))
            ns_ref[s, h] = fades[h, s : s + 1, :] * ns_ref[s, h] + kcol * written[h, s : s + 1, :]

    pltpu.make_async_copy(recv, recv, sem_recv).wait()
    for t in range(n_ep):
        rows32[t * tiles : (t + 1) * tiles, :] = recv[t].astype(F32)
    for t in range(tiles):
        lhs[:, t * LANES : (t + 1) * LANES] = rows32[pl.ds(t, n_ep, stride=tiles), :].astype(BF16)
    pushes[0].wait()
    pushes[1].wait()
    hid = []
    for p in range(2):
        g = jnp.dot(lhs[...], wg[p], preferred_element_type=F32)
        u = jnp.dot(lhs[...], wu[p], preferred_element_type=F32)
        hid.append((silu(g) * u).astype(BF16))
    pushes[2].wait()
    for t in range(tiles):
        cols = slice(t * LANES, (t + 1) * LANES)
        got = jnp.dot(hid[0], wdn[0, :, cols], preferred_element_type=F32) + jnp.dot(
            hid[1], wdn[1, :, cols], preferred_element_type=F32
        )
        term32[pl.ds(t, n_ep, stride=tiles), :] = got
    for i in range(n_ep // 2):
        for hh in range(2):
            for s in range(2):
                at = (s * (n_ep // 2) + i) * tiles + hh * htiles
                rsend[hh, i, s] = term32[at : at + htiles, :].astype(BF16)

    mine = pl.ds(2 * me, 2)
    for a, b, c in order[:-1]:
        if c % 2:
            continue
        d = zs[a] + ys[b] + xp[c]
        for hh in range(2):
            pltpu.make_async_remote_copy(
                rsend.at[hh, d // 2], ret.at[mine], sem_back, sem_home, device_id={"ep": d, "tp": hh}, device_id_type=MESH
            ).start()
    near = zs[0] + ys[0] + xp[0]
    back_other = pltpu.make_async_remote_copy(
        rsend.at[other, near // 2], ret.at[mine], sem_bself.at[0], sem_home,
        device_id={"ep": near, "tp": other}, device_id_type=MESH,
    )
    back_other.start()
    back_local = pltpu.make_async_copy(rsend.at[core, near // 2], ret.at[mine], sem_home)
    back_near = pltpu.make_async_remote_copy(
        rsend.at[core, near // 2], ret.at[mine], sem_bself.at[1], sem_home,
        device_id={"ep": near, "tp": core}, device_id_type=MESH,
    )

    @pl.when(par == core)
    def _():
        back_local.start()

    @pl.when(par != core)
    def _():
        back_near.start()

    pltpu.make_async_copy(send.at[pl.ds(0, n_ep - 1)], send.at[pl.ds(0, n_ep - 1)], sem_send).wait()

    @pl.when(par != core)
    def _():
        self_push.wait_send()

    pltpu.make_async_copy(
        rsend.at[:, pl.ds(0, n_ep // 2 - 1)], rsend.at[:, pl.ds(0, n_ep // 2 - 1)], sem_back
    ).wait()
    back_other.wait_send()

    @pl.when(par != core)
    def _():
        back_near.wait_send()

    pltpu.make_async_copy(ret, ret, sem_home).wait()
    for t in range(2 * n_ep):
        ret32[t] = ret[t].astype(F32)
    for t in range(seqs):
        acc = None
        for j in range(2):
            one = ret32[tab[2 + j, t]] * rw[j, t]
            acc = one if acc is None else acc + one
        acc32[t * htiles : (t + 1) * htiles, :] = acc
    for t in range(htiles):
        cols = slice(t * LANES, (t + 1) * LANES)
        out_ref[:, cols] = (res[:, cols] + acc32[pl.ds(t, seqs, stride=htiles), :]).astype(BF16)


def write_kernel(out_v, ns_v, out_h, ns_h, sem):
    parts = 4
    step = ns_v.shape[0] // parts
    copies = [pltpu.make_async_copy(out_v, out_h, sem.at[parts])] + [
        pltpu.make_async_copy(ns_v.at[pl.ds(i * step, step)], ns_h.at[pl.ds(i * step, step)], sem.at[i])
        for i in range(parts)
    ]
    for c in copies:
        c.start()
    for c in copies:
        c.wait()


HBM = pl.BlockSpec(memory_space=pltpu.HBM)
VMEM = pl.BlockSpec(memory_space=pltpu.VMEM)


def keep(a):
    return pltpu.with_memory_space_constraint(a, pltpu.HBM)


def per_device(
    dims,
    tokens, attn_gain, w_query, w_key, w_value, w_zgate, w_decay, w_beta, decay_rate, decay_bias,
    state, out_gain, w_out, ffn_gain, expert_gate, expert_up, expert_down, routes, route_weight,
):
    seqs, width = tokens.shape
    heads, hd = state.shape[1], state.shape[2]
    n_ep = lax.axis_size("ep")
    tiles = width // LANES
    hidden = expert_gate.shape[2]
    dma = pltpu.SemaphoreType.DMA
    smem, vmem = pltpu.SMEM, pltpu.VMEM

    args = (
        tokens, attn_gain.reshape(1, width), w_query, w_key, w_value, w_zgate, w_decay.T, w_beta.T, decay_rate,
        decay_bias, state, out_gain.reshape(1, hd), w_out, ffn_gain.reshape(1, width), expert_gate[0], expert_up[0],
        expert_down[0], routes.T, route_weight.T,
    )
    layer_out, new_state = pl.pallas_call(
        functools.partial(layer_kernel, n_ep, dims),
        name="layer",
        out_shape=(vmem((seqs, width // 2), BF16), vmem(state.shape, F32)),
        in_specs=[HBM] * len(args),
        out_specs=(VMEM, VMEM),
        scratch_shapes=[
            vmem((seqs, width), BF16),
            vmem((1, width), F32),
            vmem((heads, width, 4 * hd), BF16),
            vmem((heads, width), BF16),
            vmem((heads, width), BF16),
            smem((heads,), F32),
            smem((heads,), F32),
            vmem((1, hd), F32),
            vmem(w_out.shape, BF16),
            vmem((1, width), F32),
            vmem((2, seqs), jnp.int32),
            smem((2, seqs), F32),
            vmem((8, LANES), jnp.int32),
            smem((8, LANES), jnp.int32),
            vmem((heads, hd, seqs), F32),
            vmem((heads, seqs, hd), F32),
            vmem((heads, seqs, hd), F32),
            vmem((seqs, heads * hd), BF16),
            vmem((2, width, hidden), BF16),
            vmem((2, width, hidden), BF16),
            vmem((2, hidden, width), BF16),
            vmem((seqs, width), BF16),
            vmem((seqs, width), BF16),
            vmem((seqs * tiles, LANES), F32),
            vmem((seqs, tiles, LANES), BF16),
            vmem((n_ep, tiles, LANES), BF16),
            vmem((n_ep, tiles, LANES), BF16),
            vmem((n_ep * tiles, LANES), F32),
            vmem((n_ep, width), BF16),
            vmem((n_ep * tiles, LANES), F32),
            vmem((2, n_ep // 2, 2, tiles // 2, LANES), BF16),
            vmem((2 * n_ep, tiles // 2, LANES), BF16),
            vmem((2 * n_ep, tiles // 2, LANES), F32),
            vmem((seqs * tiles // 2, LANES), F32),
            vmem((seqs, width // 2), F32),
            dma((10,)), dma((heads, 4)), dma((heads,)), dma, dma, dma((3,)), dma((2,)), dma((3,)), dma((3,)),
            dma, dma, dma, dma, dma, dma((2,)),
        ],
        compiler_params=pltpu.CompilerParams(
            collective_id=0, has_side_effects=True, vmem_limit_bytes=40 * 2**20
        ),
    )(*[keep(a) for a in args])
    return pl.pallas_call(
        write_kernel,
        name="write",
        out_shape=(jax.ShapeDtypeStruct(layer_out.shape, BF16), jax.ShapeDtypeStruct(state.shape, F32)),
        in_specs=[VMEM, VMEM],
        out_specs=(HBM, HBM),
        scratch_shapes=[dma((5,))],
        compiler_params=pltpu.CompilerParams(vmem_limit_bytes=2**20),
    )(*[pltpu.with_memory_space_constraint(a, pltpu.VMEM) for a in (layer_out, new_state)])


def solution(mesh):
    in_specs = (
        P("ep", None), P(), P(None, "tp"), P(None, "tp"), P(None, "tp"), P(None, "tp"), P(None, "tp"), P(None, "tp"),
        P("tp"), P("tp"), P("ep", "tp", None, None), P(), P("tp", None), P(), P("ep", None, "tp"), P("ep", None, "tp"),
        P("ep", "tp", None), P("ep", None), P("ep", None),
    )
    out_specs = (P("ep", "tp"), P("ep", "tp", None, None))
    side = round(mesh.shape["ep"] ** (1 / 3))
    dims = (side, side, side)
    return jax.shard_map(
        functools.partial(per_device, dims), mesh=mesh, in_specs=in_specs, out_specs=out_specs, check_vma=False
    )
```

```python
import functools

import jax
import jax.numpy as jnp
from jax import lax
from jax.experimental import pallas as pl
from jax.experimental.pallas import tpu as pltpu
from jax.sharding import PartitionSpec as P

EPS = 1e-06
F32 = jnp.float32
BF16 = jnp.bfloat16
MESH = pl.DeviceIdType.MESH
LANES = 128


def rms_scale(rows, gain):
    return rows * lax.rsqrt(jnp.mean(rows * rows, axis=-1, keepdims=True) + EPS) * gain


def unit_rows(rows):
    return rows * lax.rsqrt(jnp.sum(rows * rows, axis=-1, keepdims=True) + EPS)


def silu(x):
    return x * (1.0 / (1.0 + jnp.exp(-x)))


def softplus(x):
    return jnp.maximum(x, 0.0) + jnp.log(1.0 + jnp.exp(-jnp.abs(x)))


def layer_kernel(
    n_ep, dims,
    tok_h, gain_h, wq_h, wk_h, wv_h, wz_h, wd_h, wb_h, rate_h, bias_h, st_h, og_h, wo_h, fgain_h, eg_h, eu_h, ed_h, rt_h, rw_h,
    out_ref, ns_ref,
    tok, gain, wbuf, wd, wb, rate, bias, og, wo, fgain, rt, rw, tab_v, tab,
    kts, written, fades, ho,
    wg, wu, wdn, mix, mix_in, moe32, moe, send, recv, rows32, lhs, term32, rsend, ret, ret32, acc32, res,
    sem_small, sem_w, sem_s, sem_wo, sem_tab, sem_e, sem_x, sem_push, sem_pull, sem_send, sem_recv, sem_self, sem_back, sem_home, sem_bself,
):
    seqs, width = tok.shape
    heads, hd = kts.shape[0], kts.shape[1]
    half = width // 2
    tiles = width // LANES
    htiles = tiles // 2
    me = lax.axis_index("ep")
    core = lax.axis_index("tp")
    other = 1 - core
    par = lax.rem(me, 2)
    shift = jnp.where(par == core, 0, 1)
    nz, ny, nx = dims

    small = [
        pltpu.make_async_copy(a, b, sem_small.at[i])
        for i, (a, b) in enumerate(
            [
                (tok_h, tok), (gain_h, gain), (wd_h, wd), (wb_h, wb), (rate_h, rate), (bias_h, bias), (og_h, og),
                (rt_h, rt), (fgain_h, fgain), (rw_h, rw),
            ]
        )
    ]
    for c in small:
        c.start()
    big = []
    for h in range(heads):
        cols = pl.ds(h * hd, hd)
        big.append(
            [
                pltpu.make_async_copy(w.at[:, cols], wbuf.at[h, :, pl.ds(i * hd, hd)], sem_w.at[h, i])
                for i, w in enumerate((wq_h, wk_h, wv_h, wz_h))
            ]
            + [pltpu.make_async_copy(st_h.at[:, h], ns_ref.at[:, h], sem_s.at[h])]
        )
    wo_in = pltpu.make_async_copy(wo_h, wo, sem_wo)
    e_in = [
        pltpu.make_async_copy(a, b.at[core], sem_e.at[i])
        for i, (a, b) in enumerate([(eg_h, wg), (eu_h, wu), (ed_h, wdn)])
    ]
    for c in big[0]:
        c.start()

    z0, y0, x0 = me // (ny * nx), lax.rem(me // nx, ny), lax.rem(me, nx)
    zs = [lax.rem(z0 + i, nz) * (ny * nx) for i in range(nz)]
    ys = [lax.rem(y0 + i, ny) * nx for i in range(ny)]
    xs = [lax.rem(x0 + i, nx) for i in range(nx)]
    xp = [lax.rem(x0 + i + shift, nx) for i in range(nx)]
    hop = lambda i, n: min(i, n - i)
    order = sorted(
        [(a, b, c) for a in range(nz) for b in range(ny) for c in range(nx)],
        key=lambda o: -(hop(o[0], nz) + hop(o[1], ny) + hop(o[2], nx)),
    )
    partner = {"ep": me, "tp": other}

    barrier = pltpu.get_barrier_semaphore()
    for a, b, c in order[:-1]:
        pl.semaphore_signal(
            barrier, inc=1, device_id={"ep": zs[a] + ys[b] + xs[c], "tp": par}, device_id_type=MESH
        )
        if c % 2 == 0:
            pl.semaphore_signal(
                barrier, inc=1, device_id={"ep": zs[a] + ys[b] + xp[c], "tp": 1 - par}, device_id_type=MESH
            )

    @pl.when(par != core)
    def _():
        pl.semaphore_signal(
            barrier, inc=1, device_id={"ep": zs[0] + ys[0] + xp[0], "tp": 1 - par}, device_id_type=MESH
        )

    pl.semaphore_signal(barrier, inc=1, device_id=partner, device_id_type=MESH)

    for c in big[1]:
        c.start()
    for c in small:
        c.wait()

    ids = lax.broadcasted_iota(jnp.int32, (n_ep, seqs), 0)
    row = lax.broadcasted_iota(jnp.int32, (n_ep, seqs), 1)
    r = rt[...]
    hits = [ids == r[j : j + 1, :] for j in range(2)]
    either = hits[0] | hits[1]
    first = jnp.min(jnp.where(either, row, seqs), axis=1, keepdims=True)
    last = jnp.max(jnp.where(either, row, 0), axis=1, keepdims=True)
    first_row = jnp.where(first == seqs, 0, first)
    diag = lax.broadcasted_iota(jnp.int32, (n_ep, n_ep), 0) == lax.broadcasted_iota(jnp.int32, (n_ep, n_ep), 1)
    tab_v[0:1, 0:n_ep] = jnp.sum(jnp.where(diag, first_row, 0), axis=0, keepdims=True)
    tab_v[1:2, 0:n_ep] = jnp.sum(jnp.where(diag, last, 0), axis=0, keepdims=True)
    later = jnp.where(row > first, 1, 0)
    for j in range(2):
        slot = jnp.sum(jnp.where(hits[j], later, 0), axis=0, keepdims=True)
        tab_v[2 + j : 3 + j, 0:seqs] = r[j : j + 1, :] * 2 + slot

    x = tok[...].astype(F32)
    normed = rms_scale(x, gain[...]).astype(BF16)
    normed32 = normed.astype(F32)

    def narrow(w, h):
        got = jnp.sum(normed32 * w[h : h + 1, :].astype(F32), axis=1, keepdims=True)
        return got.astype(BF16).astype(F32)

    betas = []
    for h in range(heads):
        fade = jnp.exp(-rate[h] * softplus(narrow(wd, h) + bias[h]))
        fades[h] = jnp.broadcast_to(fade, (seqs, hd))
        betas.append(jnp.broadcast_to(1.0 / (1.0 + jnp.exp(-narrow(wb, h))), (seqs, hd)))

    tab_copy = pltpu.make_async_copy(tab_v, tab, sem_tab)
    tab_copy.start()

    sub = lax.broadcasted_iota(jnp.int32, (8, hd), 0)
    for h in range(heads):
        for c in big[h][:4]:
            c.wait()
        if h + 2 < heads:
            for c in big[h + 2]:
                c.start()
        if h + 2 == heads:
            wo_in.start()
        if h + 1 == heads:
            for c in e_in:
                c.start()
        raw = jnp.dot(normed, wbuf[h], preferred_element_type=F32).astype(BF16).astype(F32)
        q = unit_rows(silu(raw[:, 0:hd])) * hd ** (-0.5)
        k = unit_rows(silu(raw[:, hd : 2 * hd]))
        v = silu(raw[:, 2 * hd : 3 * hd])
        z = silu(raw[:, 3 * hd : 4 * hd])
        kq = jnp.sum(k * q, axis=1, keepdims=True)
        kts[h] = k.T
        big[h][4].wait()
        preds, sqs = [], []
        for g in range(seqs // 8):
            pair = jnp.concatenate([k[g * 8 : g * 8 + 8], q[g * 8 : g * 8 + 8]], axis=0).astype(BF16)
            pred = sq = None
            for s in range(0, 8, 2):
                both = jnp.concatenate([ns_ref[g * 8 + s, h], ns_ref[g * 8 + s + 1, h]], axis=1).astype(BF16)
                got = jnp.dot(pair, both, preferred_element_type=F32)
                for i in range(2):
                    one, two = got[0:8, i * hd : (i + 1) * hd], got[8:16, i * hd : (i + 1) * hd]
                    pred = one if pred is None else jnp.where(sub == s + i, one, pred)
                    sq = two if sq is None else jnp.where(sub == s + i, two, sq)
            preds.append(pred)
            sqs.append(sq)
        pred, sq = jnp.concatenate(preds, axis=0), jnp.concatenate(sqs, axis=0)
        fade = fades[h]
        wr = betas[h] * (v - fade * pred)
        written[h] = wr
        read = fade * sq + kq * wr
        ho[:, h * hd : (h + 1) * hd] = (rms_scale(read, og[...]) * z).astype(BF16)

    wo_in.wait()
    mix[...] = jnp.dot(ho[...], wo[...], preferred_element_type=F32).astype(BF16)
    pl.semaphore_wait(barrier, 95 + shift)

    xchg = pltpu.make_async_remote_copy(
        mix, mix_in, sem_x.at[0], sem_x.at[1], device_id=partner, device_id_type=MESH
    )
    xchg.start()
    pushes = [
        pltpu.make_async_remote_copy(
            b.at[core], b.at[core], sem_push.at[i], sem_pull.at[i], device_id=partner, device_id_type=MESH
        )
        for i, b in enumerate((wg, wu, wdn))
    ]
    e_in[0].wait()
    pushes[0].start()
    tab_copy.wait()
    xchg.wait()

    resid = tok[...].astype(F32) + (mix[...].astype(F32) + mix_in[...].astype(F32))
    moe_in = rms_scale(resid, fgain[...])
    for t in range(tiles):
        moe32[pl.ds(t, seqs, stride=tiles), :] = moe_in[:, t * LANES : (t + 1) * LANES]

    @pl.when(core == 0)
    def _():
        res[...] = resid[:, :half]

    @pl.when(core == 1)
    def _():
        res[...] = resid[:, half:]

    for t in range(seqs):
        moe[t] = moe32[t * tiles : (t + 1) * tiles, :].astype(BF16)
    targets = [(a, b, c) for a, b, c in order if c % 2 == 0]
    dest = [zs[a] + ys[b] + xp[c] for a, b, c in targets]
    count = len(dest)
    pair = lambda i: pl.ds(2 * i, 2)
    for i in range(count):
        for slot in range(2):
            send[2 * i + slot] = moe[tab[slot, dest[i]]]
    group = z0 // (nz // 2)
    landing = recv.at[pair(me // 2)]
    for i in range(count - 1):
        pltpu.make_async_remote_copy(
            send.at[pair(i)], landing, sem_send, sem_recv.at[group],
            device_id={"ep": dest[i], "tp": par}, device_id_type=MESH,
        ).start()
    end = count - 1
    end_far = pltpu.make_async_remote_copy(
        send.at[pair(end)], landing, sem_self, sem_recv.at[group],
        device_id={"ep": dest[end], "tp": par}, device_id_type=MESH,
    )
    end_local = pltpu.make_async_copy(send.at[pair(end)], landing, sem_recv.at[group])

    @pl.when(par != core)
    def _():
        end_far.start()

    @pl.when(par == core)
    def _():
        end_local.start()

    for i in (1, 2):
        e_in[i].wait()
        pushes[i].start()

    for h in range(heads):
        for s in range(seqs):
            kcol = jnp.broadcast_to(kts[h, :, s : s + 1], (hd, hd))
            ns_ref[s, h] = fades[h, s : s + 1, :] * ns_ref[s, h] + kcol * written[h, s : s + 1, :]

    place = pl.ds(2 * me, 2)
    rows = n_ep // 2
    flat = sorted([(b, c) for b in range(ny) for c in range(0, nx, 2)], key=lambda o: -(hop(o[0], ny) + hop(o[1], nx)))
    locals_ = []
    for g in range(2):
        here = recv.at[pl.ds(rows * g, rows)]
        pltpu.make_async_copy(here, here, sem_recv.at[g]).wait()
        for t in range(rows):
            rows32[t * tiles : (t + 1) * tiles, :] = recv[rows * g + t].astype(F32)
        for t in range(tiles):
            lhs[:, t * LANES : (t + 1) * LANES] = rows32[pl.ds(t, rows, stride=tiles), :].astype(BF16)
        if g == 0:
            pushes[0].wait()
            pushes[1].wait()
        hid = []
        for p in range(2):
            gate = jnp.dot(lhs[...], wg[p], preferred_element_type=F32)
            up = jnp.dot(lhs[...], wu[p], preferred_element_type=F32)
            hid.append((silu(gate) * up).astype(BF16))
        if g == 0:
            pushes[2].wait()
        for t in range(tiles):
            cols = slice(t * LANES, (t + 1) * LANES)
            got = jnp.dot(hid[0], wdn[0, :, cols], preferred_element_type=F32) + jnp.dot(
                hid[1], wdn[1, :, cols], preferred_element_type=F32
            )
            term32[pl.ds(t, rows, stride=tiles), :] = got
        for i in range(rows // 2):
            for hh in range(2):
                for slot in range(2):
                    at = (2 * i + slot) * tiles + hh * htiles
                    rsend[hh, g * (rows // 2) + i, slot] = term32[at : at + htiles, :].astype(BF16)

        for b, c in flat:
            for z in range(g * nz // 2, (g + 1) * nz // 2):
                d = z * (ny * nx) + ys[b] + xp[c]
                if b or c:
                    for hh in range(2):
                        pltpu.make_async_remote_copy(
                            rsend.at[hh, d // 2], ret.at[place], sem_back, sem_home,
                            device_id={"ep": d, "tp": hh}, device_id_type=MESH,
                        ).start()
                else:
                    pltpu.make_async_remote_copy(
                        rsend.at[other, d // 2], ret.at[place], sem_back, sem_home,
                        device_id={"ep": d, "tp": other}, device_id_type=MESH,
                    ).start()
                    stays = (z == z0) & (par == core)
                    back_far = pltpu.make_async_remote_copy(
                        rsend.at[core, d // 2], ret.at[place], sem_bself.at[z], sem_home,
                        device_id={"ep": d, "tp": core}, device_id_type=MESH,
                    )
                    back_local = pltpu.make_async_copy(rsend.at[core, d // 2], ret.at[place], sem_home)
                    locals_.append((stays, back_far))

                    @pl.when(stays)
                    def _():
                        back_local.start()

                    @pl.when(jnp.logical_not(stays))
                    def _():
                        back_far.start()

    sent = send.at[pl.ds(0, 2 * count - 2)]
    pltpu.make_async_copy(sent, sent, sem_send).wait()

    @pl.when(par != core)
    def _():
        end_far.wait_send()

    sent = rsend.at[:, pl.ds(0, count - nz // 2)]
    pltpu.make_async_copy(sent, sent, sem_back).wait()
    for stays, back_far in locals_:

        @pl.when(jnp.logical_not(stays))
        def _():
            back_far.wait_send()

    pltpu.make_async_copy(ret, ret, sem_home).wait()
    for t in range(2 * n_ep):
        ret32[t] = ret[t].astype(F32)
    for t in range(seqs):
        acc = None
        for j in range(2):
            one = ret32[tab[2 + j, t]] * rw[j, t]
            acc = one if acc is None else acc + one
        acc32[t * htiles : (t + 1) * htiles, :] = acc
    for t in range(htiles):
        cols = slice(t * LANES, (t + 1) * LANES)
        out_ref[:, cols] = (res[:, cols] + acc32[pl.ds(t, seqs, stride=htiles), :]).astype(BF16)


def write_kernel(out_v, ns_v, out_h, ns_h, sem):
    parts = 4
    step = ns_v.shape[0] // parts
    copies = [pltpu.make_async_copy(out_v, out_h, sem.at[parts])] + [
        pltpu.make_async_copy(ns_v.at[pl.ds(i * step, step)], ns_h.at[pl.ds(i * step, step)], sem.at[i])
        for i in range(parts)
    ]
    for c in copies:
        c.start()
    for c in copies:
        c.wait()


HBM = pl.BlockSpec(memory_space=pltpu.HBM)
VMEM = pl.BlockSpec(memory_space=pltpu.VMEM)


def keep(a):
    return pltpu.with_memory_space_constraint(a, pltpu.HBM)


def per_device(
    dims,
    tokens, attn_gain, w_query, w_key, w_value, w_zgate, w_decay, w_beta, decay_rate, decay_bias,
    state, out_gain, w_out, ffn_gain, expert_gate, expert_up, expert_down, routes, route_weight,
):
    seqs, width = tokens.shape
    heads, hd = state.shape[1], state.shape[2]
    n_ep = lax.axis_size("ep")
    tiles = width // LANES
    hidden = expert_gate.shape[2]
    dma = pltpu.SemaphoreType.DMA
    smem, vmem = pltpu.SMEM, pltpu.VMEM

    args = (
        tokens, attn_gain.reshape(1, width), w_query, w_key, w_value, w_zgate, w_decay.T, w_beta.T, decay_rate,
        decay_bias, state, out_gain.reshape(1, hd), w_out, ffn_gain.reshape(1, width), expert_gate[0], expert_up[0],
        expert_down[0], routes.T, route_weight.T,
    )
    layer_out, new_state = pl.pallas_call(
        functools.partial(layer_kernel, n_ep, dims),
        name="layer",
        out_shape=(vmem((seqs, width // 2), BF16), vmem(state.shape, F32)),
        in_specs=[HBM] * len(args),
        out_specs=(VMEM, VMEM),
        scratch_shapes=[
            vmem((seqs, width), BF16),
            vmem((1, width), F32),
            vmem((heads, width, 4 * hd), BF16),
            vmem((heads, width), BF16),
            vmem((heads, width), BF16),
            smem((heads,), F32),
            smem((heads,), F32),
            vmem((1, hd), F32),
            vmem(w_out.shape, BF16),
            vmem((1, width), F32),
            vmem((2, seqs), jnp.int32),
            smem((2, seqs), F32),
            vmem((8, LANES), jnp.int32),
            smem((8, LANES), jnp.int32),
            vmem((heads, hd, seqs), F32),
            vmem((heads, seqs, hd), F32),
            vmem((heads, seqs, hd), F32),
            vmem((seqs, heads * hd), BF16),
            vmem((2, width, hidden), BF16),
            vmem((2, width, hidden), BF16),
            vmem((2, hidden, width), BF16),
            vmem((seqs, width), BF16),
            vmem((seqs, width), BF16),
            vmem((seqs * tiles, LANES), F32),
            vmem((seqs, tiles, LANES), BF16),
            vmem((n_ep, tiles, LANES), BF16),
            vmem((n_ep, tiles, LANES), BF16),
            vmem((n_ep // 2 * tiles, LANES), F32),
            vmem((n_ep // 2, width), BF16),
            vmem((n_ep // 2 * tiles, LANES), F32),
            vmem((2, n_ep // 2, 2, tiles // 2, LANES), BF16),
            vmem((2 * n_ep, tiles // 2, LANES), BF16),
            vmem((2 * n_ep, tiles // 2, LANES), F32),
            vmem((seqs * tiles // 2, LANES), F32),
            vmem((seqs, width // 2), F32),
            dma((10,)), dma((heads, 4)), dma((heads,)), dma, dma, dma((3,)), dma((2,)), dma((3,)), dma((3,)),
            dma, dma((2,)), dma, dma, dma, dma((dims[0],)),
        ],
        compiler_params=pltpu.CompilerParams(
            collective_id=0, has_side_effects=True, vmem_limit_bytes=40 * 2**20
        ),
    )(*[keep(a) for a in args])
    return pl.pallas_call(
        write_kernel,
        name="write",
        out_shape=(jax.ShapeDtypeStruct(layer_out.shape, BF16), jax.ShapeDtypeStruct(state.shape, F32)),
        in_specs=[VMEM, VMEM],
        out_specs=(HBM, HBM),
        scratch_shapes=[dma((5,))],
        compiler_params=pltpu.CompilerParams(vmem_limit_bytes=2**20),
    )(*[pltpu.with_memory_space_constraint(a, pltpu.VMEM) for a in (layer_out, new_state)])


def solution(mesh):
    in_specs = (
        P("ep", None), P(), P(None, "tp"), P(None, "tp"), P(None, "tp"), P(None, "tp"), P(None, "tp"), P(None, "tp"),
        P("tp"), P("tp"), P("ep", "tp", None, None), P(), P("tp", None), P(), P("ep", None, "tp"), P("ep", None, "tp"),
        P("ep", "tp", None), P("ep", None), P("ep", None),
    )
    out_specs = (P("ep", "tp"), P("ep", "tp", None, None))
    side = round(mesh.shape["ep"] ** (1 / 3))
    dims = (side, side, side)
    return jax.shard_map(
        functools.partial(per_device, dims), mesh=mesh, in_specs=in_specs, out_specs=out_specs, check_vma=False
    )
```

```python
import functools

import jax
import jax.numpy as jnp
from jax import lax
from jax.experimental import pallas as pl
from jax.experimental.pallas import tpu as pltpu
from jax.sharding import PartitionSpec as P

EPS = 1e-06
F32 = jnp.float32
BF16 = jnp.bfloat16
MESH = pl.DeviceIdType.MESH
LANES = 128


def rms_scale(rows, gain):
    return rows * lax.rsqrt(jnp.mean(rows * rows, axis=-1, keepdims=True) + EPS) * gain


def unit_rows(rows):
    return rows * lax.rsqrt(jnp.sum(rows * rows, axis=-1, keepdims=True) + EPS)


def silu(x):
    return x * (1.0 / (1.0 + jnp.exp(-x)))


def softplus(x):
    return jnp.maximum(x, 0.0) + jnp.log(1.0 + jnp.exp(-jnp.abs(x)))


def split_plane(ny, nx):
    hops = lambda o: min(o[0], ny - o[0]) + min(o[1], nx - o[1])
    back = lambda o: (-o[0] % ny, -o[1] % nx)
    every = [(b, c) for b in range(ny) for c in range(nx)]
    every.sort(key=lambda o: (-hops(o), o == back(o), min(o, back(o))))
    half = len(every) // 2
    far, near = every[:half], every[half:]
    if any(back(o) not in far for o in far):
        odd = next(o for o in far if back(o) not in far)
        own = next(o for o in near if o == back(o) and any(o))
        far[far.index(odd)], near[near.index(own)] = own, odd
    assert all(back(o) in far for o in far)
    return far, near


CUTS = (0, 1, 2, 4)


def layer_kernel(
    n_ep, dims,
    tok_h, gain_h, wq_h, wk_h, wv_h, wz_h, wd_h, wb_h, rate_h, bias_h, st_h, og_h, wo_h, fgain_h, eg_h, eu_h, ed_h, rt_h, rw_h,
    out_ref, ns_ref,
    tok, gain, wbuf, wd, wb, rate, bias, og, wo, fgain, rt, rw, tab_v, tab,
    kts, written, fades, ho, mix32,
    wg, wu, wdn, mix, mix_in, moe32, moe, send, recv, rows32, lhs, term32, rsend, ret, ret32, acc32, res,
    sem_small, sem_w, sem_s, sem_wo, sem_tab, sem_e, sem_x, sem_push, sem_pull, sem_send, sem_recv, sem_self, sem_back, sem_home, sem_bself,
):
    seqs, width = tok.shape
    heads, hd = kts.shape[0], kts.shape[1]
    half = width // 2
    tiles = width // LANES
    htiles = tiles // 2
    me = lax.axis_index("ep")
    core = lax.axis_index("tp")
    other = 1 - core
    nz, ny, nx = dims

    small = [
        pltpu.make_async_copy(a, b, sem_small.at[i])
        for i, (a, b) in enumerate(
            [
                (tok_h, tok), (gain_h, gain), (wd_h, wd), (wb_h, wb), (rate_h, rate), (bias_h, bias), (og_h, og),
                (rt_h, rt), (fgain_h, fgain), (rw_h, rw),
            ]
        )
    ]
    for c in small:
        c.start()
    big = []
    for h in range(heads):
        cols = pl.ds(h * hd, hd)
        big.append(
            [
                pltpu.make_async_copy(w.at[:, cols], wbuf.at[h, :, pl.ds(i * hd, hd)], sem_w.at[h, i])
                for i, w in enumerate((wq_h, wk_h, wv_h, wz_h))
            ]
            + [pltpu.make_async_copy(st_h.at[:, h], ns_ref.at[:, h], sem_s.at[h])]
        )
    wo_in = pltpu.make_async_copy(wo_h, wo, sem_wo)
    e_in = [
        pltpu.make_async_copy(a, b.at[core], sem_e.at[i])
        for i, (a, b) in enumerate([(eg_h, wg), (eu_h, wu), (ed_h, wdn)])
    ]
    units = []
    for h in range(heads):
        units.append(big[h][:4])
        if h + 1 == heads:
            units.append([wo_in])
        units.append(big[h][4:])
    units += [e_in, [], [], []]
    for u in units[:2]:
        for c in u:
            c.start()

    def take(n):
        for c in units[n]:
            c.wait()
        for c in units[n + 4]:
            c.start()

    z0, y0, x0 = me // (ny * nx), lax.rem(me // nx, ny), lax.rem(me, nx)
    zs = [lax.rem(z0 + i, nz) * (ny * nx) for i in range(nz)]
    ys = [lax.rem(y0 + i, ny) * nx for i in range(ny)]
    xs = [lax.rem(x0 + i, nx) for i in range(nx)]
    far, near = split_plane(ny, nx)
    count = len(far)
    ahead = lambda o: ys[o[0]] + xs[o[1]]
    behind = lambda o: ys[-o[0] % ny] + xs[-o[1] % nx]
    mine = [jnp.where(core == 1, ahead(f), ahead(n)) for f, n in zip(far, near)]
    their = [jnp.where(core == 1, ahead(n), ahead(f)) for f, n in zip(far, near)]
    home = [jnp.where(core == 1, behind(f), behind(n)) for f, n in zip(far, near)]
    hop = lambda i, n: min(i, n - i)
    order = sorted(
        [(a, j) for a in range(nz) for j in range(count)],
        key=lambda o: (-(hop(o[0], nz) + hop(far[o[1]][0], ny) + hop(far[o[1]][1], nx)), -o[0]),
    )
    order.remove((0, count - 1))
    order.append((0, count - 1))
    partner = {"ep": me, "tp": other}

    barrier = pltpu.get_barrier_semaphore()
    for a, j in order[:-1]:
        pl.semaphore_signal(barrier, inc=1, device_id={"ep": zs[a] + mine[j], "tp": core}, device_id_type=MESH)
        pl.semaphore_signal(barrier, inc=1, device_id={"ep": zs[a] + mine[j], "tp": other}, device_id_type=MESH)
        pl.semaphore_signal(barrier, inc=1, device_id={"ep": zs[a] + their[j], "tp": other}, device_id_type=MESH)
    last = zs[0] + mine[count - 1]

    @pl.when(core == 1)
    def _():
        pl.semaphore_signal(barrier, inc=1, device_id={"ep": last, "tp": core}, device_id_type=MESH)

    pl.semaphore_signal(barrier, inc=1, device_id={"ep": last, "tp": other}, device_id_type=MESH)
    pl.semaphore_signal(barrier, inc=1, device_id={"ep": zs[0] + their[count - 1], "tp": other}, device_id_type=MESH)

    for u in units[2:4]:
        for c in u:
            c.start()
    for c in small:
        c.wait()

    ids = lax.broadcasted_iota(jnp.int32, (n_ep, seqs), 0)
    row = lax.broadcasted_iota(jnp.int32, (n_ep, seqs), 1)
    r = rt[...]
    hits = [ids == r[j : j + 1, :] for j in range(2)]
    either = hits[0] | hits[1]
    first = jnp.min(jnp.where(either, row, seqs), axis=1, keepdims=True)
    final = jnp.max(jnp.where(either, row, 0), axis=1, keepdims=True)
    first_row = jnp.where(first == seqs, 0, first)
    diag = lax.broadcasted_iota(jnp.int32, (n_ep, n_ep), 0) == lax.broadcasted_iota(jnp.int32, (n_ep, n_ep), 1)
    tab_v[0:1, 0:n_ep] = jnp.sum(jnp.where(diag, first_row, 0), axis=0, keepdims=True)
    tab_v[1:2, 0:n_ep] = jnp.sum(jnp.where(diag, final, 0), axis=0, keepdims=True)
    later = jnp.where(row > first, 1, 0)
    for j in range(2):
        slot = jnp.sum(jnp.where(hits[j], later, 0), axis=0, keepdims=True)
        tab_v[2 + j : 3 + j, 0:seqs] = r[j : j + 1, :] * 2 + slot

    x = tok[...].astype(F32)
    normed = rms_scale(x, gain[...]).astype(BF16)
    normed32 = normed.astype(F32)

    def narrow(w, h):
        got = jnp.sum(normed32 * w[h : h + 1, :].astype(F32), axis=1, keepdims=True)
        return got.astype(BF16).astype(F32)

    betas = []
    for h in range(heads):
        fade = jnp.exp(-rate[h] * softplus(narrow(wd, h) + bias[h]))
        fades[h] = jnp.broadcast_to(fade, (seqs, hd))
        betas.append(jnp.broadcast_to(1.0 / (1.0 + jnp.exp(-narrow(wb, h))), (seqs, hd)))

    tab_copy = pltpu.make_async_copy(tab_v, tab, sem_tab)
    tab_copy.start()

    sub = lax.broadcasted_iota(jnp.int32, (8, hd), 0)

    def project(h):
        return jnp.dot(normed, wbuf[h], preferred_element_type=F32).astype(BF16).astype(F32)

    def mixing(h, raw):
        q = unit_rows(silu(raw[:, 0:hd])) * hd ** (-0.5)
        k = unit_rows(silu(raw[:, hd : 2 * hd]))
        v = silu(raw[:, 2 * hd : 3 * hd])
        z = silu(raw[:, 3 * hd : 4 * hd])
        kq = jnp.sum(k * q, axis=1, keepdims=True)
        kts[h] = k.T
        preds, sqs = [], []
        for g in range(seqs // 8):
            both = jnp.concatenate([k[g * 8 : g * 8 + 8], q[g * 8 : g * 8 + 8]], axis=0).astype(BF16)
            pred = sq = None
            for s in range(0, 8, 2):
                two = jnp.concatenate([ns_ref[g * 8 + s, h], ns_ref[g * 8 + s + 1, h]], axis=1).astype(BF16)
                got = jnp.dot(both, two, preferred_element_type=F32)
                for i in range(2):
                    top, low = got[0:8, i * hd : (i + 1) * hd], got[8:16, i * hd : (i + 1) * hd]
                    pred = top if pred is None else jnp.where(sub == s + i, top, pred)
                    sq = low if sq is None else jnp.where(sub == s + i, low, sq)
            preds.append(pred)
            sqs.append(sq)
        pred, sq = jnp.concatenate(preds, axis=0), jnp.concatenate(sqs, axis=0)
        fade = fades[h]
        wr = betas[h] * (v - fade * pred)
        written[h] = wr
        read = fade * sq + kq * wr
        ho[:, h * hd : (h + 1) * hd] = (rms_scale(read, og[...]) * z).astype(BF16)

    early = (heads - 1) * hd
    take(0)
    raw = project(0)
    for h in range(heads - 1):
        take(2 * h + 1)
        take(2 * h + 2)
        after = project(h + 1)
        mixing(h, raw)
        raw = after
    take(2 * heads - 1)
    mix32[...] = jnp.dot(ho[:, :early], wo[:early], preferred_element_type=F32)
    take(2 * heads)
    mixing(heads - 1, raw)
    mix[...] = (mix32[...] + jnp.dot(ho[:, early:], wo[early:], preferred_element_type=F32)).astype(BF16)
    pl.semaphore_wait(barrier, 3 * nz * count - 1 + core)

    xchg = pltpu.make_async_remote_copy(
        mix, mix_in, sem_x.at[0], sem_x.at[1], device_id=partner, device_id_type=MESH
    )
    xchg.start()
    pushes = [
        pltpu.make_async_remote_copy(
            b.at[core], b.at[core], sem_push.at[i], sem_pull.at[i], device_id=partner, device_id_type=MESH
        )
        for i, b in enumerate((wg, wu, wdn))
    ]
    e_in[0].wait()
    pushes[0].start()
    tab_copy.wait()
    xchg.wait()

    resid = tok[...].astype(F32) + (mix[...].astype(F32) + mix_in[...].astype(F32))
    moe_in = rms_scale(resid, fgain[...])
    for t in range(tiles):
        moe32[pl.ds(t, seqs, stride=tiles), :] = moe_in[:, t * LANES : (t + 1) * LANES]

    @pl.when(core == 0)
    def _():
        res[...] = resid[:, :half]

    @pl.when(core == 1)
    def _():
        res[...] = resid[:, half:]

    for t in range(seqs):
        moe[t] = moe32[t * tiles : (t + 1) * tiles, :].astype(BF16)
    pair = lambda i: pl.ds(2 * i, 2)
    for i, (a, j) in enumerate(order):
        for slot in range(2):
            send[2 * i + slot] = moe[tab[slot, zs[a] + mine[j]]]
    cuts = CUTS
    group = sum(jnp.where(z0 >= cut, 1, 0) for cut in cuts[1:-1])
    end = len(order) - 1
    for i, (a, j) in enumerate(order[:-1]):
        pltpu.make_async_remote_copy(
            send.at[pair(i)], recv.at[pair(z0 * count + j)], sem_send, sem_recv.at[group],
            device_id={"ep": zs[a] + mine[j], "tp": core}, device_id_type=MESH,
        ).start()
    landing = recv.at[pair(z0 * count + count - 1)]
    end_far = pltpu.make_async_remote_copy(
        send.at[pair(end)], landing, sem_self, sem_recv.at[group], device_id={"ep": last, "tp": core}, device_id_type=MESH
    )
    end_local = pltpu.make_async_copy(send.at[pair(end)], landing, sem_recv.at[group])

    @pl.when(core == 1)
    def _():
        end_far.start()

    @pl.when(core == 0)
    def _():
        end_local.start()

    for i in (1, 2):
        e_in[i].wait()
        pushes[i].start()

    for h in range(heads):
        for s in range(seqs):
            kcol = jnp.broadcast_to(kts[h, :, s : s + 1], (hd, hd))
            ns_ref[s, h] = fades[h, s : s + 1, :] * ns_ref[s, h] + kcol * written[h, s : s + 1, :]

    place = pl.ds(2 * me, 2)
    per_z = 2 * count
    locals_ = []
    for g in range(len(cuts) - 1):
        low, rows = cuts[g] * per_z, (cuts[g + 1] - cuts[g]) * per_z
        here = recv.at[pl.ds(low, rows)]
        pltpu.make_async_copy(here, here, sem_recv.at[g]).wait()
        for t in range(rows):
            rows32[t * tiles : (t + 1) * tiles, :] = recv[low + t].astype(F32)
        for t in range(tiles):
            lhs[:rows, t * LANES : (t + 1) * LANES] = rows32[pl.ds(t, rows, stride=tiles), :].astype(BF16)
        if g == 0:
            pushes[0].wait()
            pushes[1].wait()
        hid = []
        for p in range(2):
            gate = jnp.dot(lhs[:rows], wg[p], preferred_element_type=F32)
            up = jnp.dot(lhs[:rows], wu[p], preferred_element_type=F32)
            hid.append((silu(gate) * up).astype(BF16))
        if g == 0:
            pushes[2].wait()
        for t in range(tiles):
            cols = slice(t * LANES, (t + 1) * LANES)
            got = jnp.dot(hid[0], wdn[0, :, cols], preferred_element_type=F32) + jnp.dot(
                hid[1], wdn[1, :, cols], preferred_element_type=F32
            )
            term32[pl.ds(t, rows, stride=tiles), :] = got
        for i in range(rows // 2):
            for hh in range(2):
                for slot in range(2):
                    at = (2 * i + slot) * tiles + hh * htiles
                    rsend[hh, low // 2 + i, slot] = term32[at : at + htiles, :].astype(BF16)

        for j in range(count):
            for z in range(cuts[g], cuts[g + 1]):
                d, i = z * (ny * nx) + home[j], z * count + j
                for hh in range(2):
                    if hh == 1 or j + 1 < count:
                        pltpu.make_async_remote_copy(
                            rsend.at[hh, i], ret.at[place], sem_back, sem_home,
                            device_id={"ep": d, "tp": hh}, device_id_type=MESH,
                        ).start()
                        continue
                    stays = (z == z0) & (core == 0)
                    back_far = pltpu.make_async_remote_copy(
                        rsend.at[hh, i], ret.at[place], sem_bself.at[z], sem_home,
                        device_id={"ep": d, "tp": hh}, device_id_type=MESH,
                    )
                    back_local = pltpu.make_async_copy(rsend.at[hh, i], ret.at[place], sem_home)
                    locals_.append((stays, back_far))

                    @pl.when(stays)
                    def _():
                        back_local.start()

                    @pl.when(jnp.logical_not(stays))
                    def _():
                        back_far.start()

    sent = send.at[pl.ds(0, 2 * end)]
    pltpu.make_async_copy(sent, sent, sem_send).wait()

    @pl.when(core == 1)
    def _():
        end_far.wait_send()

    sent = rsend.at[:, pl.ds(0, nz * count - nz // 2)]
    pltpu.make_async_copy(sent, sent, sem_back).wait()
    for stays, back_far in locals_:

        @pl.when(jnp.logical_not(stays))
        def _():
            back_far.wait_send()

    pltpu.make_async_copy(ret, ret, sem_home).wait()
    for t in range(2 * n_ep):
        ret32[t] = ret[t].astype(F32)
    for t in range(seqs):
        acc = None
        for j in range(2):
            one = ret32[tab[2 + j, t]] * rw[j, t]
            acc = one if acc is None else acc + one
        acc32[t * htiles : (t + 1) * htiles, :] = acc
    for t in range(htiles):
        cols = slice(t * LANES, (t + 1) * LANES)
        out_ref[:, cols] = (res[:, cols] + acc32[pl.ds(t, seqs, stride=htiles), :]).astype(BF16)


def write_kernel(out_v, ns_v, out_h, ns_h, sem):
    parts = 4
    step = ns_v.shape[0] // parts
    copies = [pltpu.make_async_copy(out_v, out_h, sem.at[parts])] + [
        pltpu.make_async_copy(ns_v.at[pl.ds(i * step, step)], ns_h.at[pl.ds(i * step, step)], sem.at[i])
        for i in range(parts)
    ]
    for c in copies:
        c.start()
    for c in copies:
        c.wait()


HBM = pl.BlockSpec(memory_space=pltpu.HBM)
VMEM = pl.BlockSpec(memory_space=pltpu.VMEM)


def keep(a):
    return pltpu.with_memory_space_constraint(a, pltpu.HBM)


def per_device(
    dims,
    tokens, attn_gain, w_query, w_key, w_value, w_zgate, w_decay, w_beta, decay_rate, decay_bias,
    state, out_gain, w_out, ffn_gain, expert_gate, expert_up, expert_down, routes, route_weight,
):
    seqs, width = tokens.shape
    heads, hd = state.shape[1], state.shape[2]
    n_ep = lax.axis_size("ep")
    tiles = width // LANES
    hidden = expert_gate.shape[2]
    dma = pltpu.SemaphoreType.DMA
    smem, vmem = pltpu.SMEM, pltpu.VMEM

    args = (
        tokens, attn_gain.reshape(1, width), w_query, w_key, w_value, w_zgate, w_decay.T, w_beta.T, decay_rate,
        decay_bias, state, out_gain.reshape(1, hd), w_out, ffn_gain.reshape(1, width), expert_gate[0], expert_up[0],
        expert_down[0], routes.T, route_weight.T,
    )
    layer_out, new_state = pl.pallas_call(
        functools.partial(layer_kernel, n_ep, dims),
        name="layer",
        out_shape=(vmem((seqs, width // 2), BF16), vmem(state.shape, F32)),
        in_specs=[HBM] * len(args),
        out_specs=(VMEM, VMEM),
        scratch_shapes=[
            vmem((seqs, width), BF16),
            vmem((1, width), F32),
            vmem((heads, width, 4 * hd), BF16),
            vmem((heads, width), BF16),
            vmem((heads, width), BF16),
            smem((heads,), F32),
            smem((heads,), F32),
            vmem((1, hd), F32),
            vmem(w_out.shape, BF16),
            vmem((1, width), F32),
            vmem((2, seqs), jnp.int32),
            smem((2, seqs), F32),
            vmem((8, LANES), jnp.int32),
            smem((8, LANES), jnp.int32),
            vmem((heads, hd, seqs), F32),
            vmem((heads, seqs, hd), F32),
            vmem((heads, seqs, hd), F32),
            vmem((seqs, heads * hd), BF16),
            vmem((seqs, width), F32),
            vmem((2, width, hidden), BF16),
            vmem((2, width, hidden), BF16),
            vmem((2, hidden, width), BF16),
            vmem((seqs, width), BF16),
            vmem((seqs, width), BF16),
            vmem((seqs * tiles, LANES), F32),
            vmem((seqs, tiles, LANES), BF16),
            vmem((n_ep, tiles, LANES), BF16),
            vmem((n_ep, tiles, LANES), BF16),
            vmem((n_ep // 2 * tiles, LANES), F32),
            vmem((n_ep // 2, width), BF16),
            vmem((n_ep // 2 * tiles, LANES), F32),
            vmem((2, n_ep // 2, 2, tiles // 2, LANES), BF16),
            vmem((2 * n_ep, tiles // 2, LANES), BF16),
            vmem((2 * n_ep, tiles // 2, LANES), F32),
            vmem((seqs * tiles // 2, LANES), F32),
            vmem((seqs, width // 2), F32),
            dma((10,)), dma((heads, 4)), dma((heads,)), dma, dma, dma((3,)), dma((2,)), dma((3,)), dma((3,)),
            dma, dma((3,)), dma, dma, dma, dma((dims[0],)),
        ],
        compiler_params=pltpu.CompilerParams(
            collective_id=0, has_side_effects=True, vmem_limit_bytes=40 * 2**20
        ),
    )(*[keep(a) for a in args])
    return pl.pallas_call(
        write_kernel,
        name="write",
        out_shape=(jax.ShapeDtypeStruct(layer_out.shape, BF16), jax.ShapeDtypeStruct(state.shape, F32)),
        in_specs=[VMEM, VMEM],
        out_specs=(HBM, HBM),
        scratch_shapes=[dma((5,))],
        compiler_params=pltpu.CompilerParams(vmem_limit_bytes=2**20),
    )(*[pltpu.with_memory_space_constraint(a, pltpu.VMEM) for a in (layer_out, new_state)])


def solution(mesh):
    in_specs = (
        P("ep", None), P(), P(None, "tp"), P(None, "tp"), P(None, "tp"), P(None, "tp"), P(None, "tp"), P(None, "tp"),
        P("tp"), P("tp"), P("ep", "tp", None, None), P(), P("tp", None), P(), P("ep", None, "tp"), P("ep", None, "tp"),
        P("ep", "tp", None), P("ep", None), P("ep", None),
    )
    out_specs = (P("ep", "tp"), P("ep", "tp", None, None))
    side = round(mesh.shape["ep"] ** (1 / 3))
    dims = (side, side, side)
    return jax.shard_map(
        functools.partial(per_device, dims), mesh=mesh, in_specs=in_specs, out_specs=out_specs, check_vma=False
    )
```

```python
import functools

import jax
import jax.numpy as jnp
from jax import lax
from jax.experimental import pallas as pl
from jax.experimental.pallas import tpu as pltpu
from jax.sharding import PartitionSpec as P

EPS = 1e-06
F32 = jnp.float32
BF16 = jnp.bfloat16
MESH = pl.DeviceIdType.MESH
LANES = 128


def rms_scale(rows, gain):
    return rows * lax.rsqrt(jnp.mean(rows * rows, axis=-1, keepdims=True) + EPS) * gain


def unit_rows(rows):
    return rows * lax.rsqrt(jnp.sum(rows * rows, axis=-1, keepdims=True) + EPS)


def silu(x):
    return x * (1.0 / (1.0 + jnp.exp(-x)))


def softplus(x):
    return jnp.maximum(x, 0.0) + jnp.log(1.0 + jnp.exp(-jnp.abs(x)))


def split_plane(ny, nx):
    hops = lambda o: min(o[0], ny - o[0]) + min(o[1], nx - o[1])
    back = lambda o: (-o[0] % ny, -o[1] % nx)
    every = [(b, c) for b in range(ny) for c in range(nx)]
    every.sort(key=lambda o: (-hops(o), o == back(o), min(o, back(o))))
    half = len(every) // 2
    far, near = every[:half], every[half:]
    if any(back(o) not in far for o in far):
        odd = next(o for o in far if back(o) not in far)
        own = next(o for o in near if o == back(o) and any(o))
        far[far.index(odd)], near[near.index(own)] = own, odd
    assert all(back(o) in far for o in far)
    return far, near


CUTS = (0, 1, 2, 4)


def layer_kernel(
    n_ep, dims,
    tok_h, gain_h, wq_h, wk_h, wv_h, wz_h, wd_h, wb_h, rate_h, bias_h, st_h, og_h, wo_h, fgain_h, eg_h, eu_h, ed_h, rt_h, rw_h,
    out_ref, ns_ref,
    tok, gain, wbuf, wd, wb, rate, bias, og, wo, fgain, rt, rw, tab_v, tab,
    kts, written, fades, ho, mix32,
    wg, wu, wdn, mix, mix_in, moe32, moe, send, recv, rows32, lhs, term32, rsend, ret, ret32, acc32, res,
    sem_small, sem_w, sem_s, sem_wo, sem_x, sem_pull, sem_recv, sem_home,
):
    seqs, width = tok.shape
    heads, hd = kts.shape[0], kts.shape[1]
    half = width // 2
    tiles = width // LANES
    htiles = tiles // 2
    me = lax.axis_index("ep")
    core = lax.axis_index("tp")
    other = 1 - core
    nz, ny, nx = dims

    small = [
        pltpu.make_async_copy(a, b, sem_small.at[i])
        for i, (a, b) in enumerate(
            [
                (tok_h, tok), (gain_h, gain), (wd_h, wd), (wb_h, wb), (rate_h, rate), (bias_h, bias), (og_h, og),
                (rt_h, rt), (fgain_h, fgain), (rw_h, rw),
            ]
        )
    ]
    for c in small:
        c.start()
    big = []
    for h in range(heads):
        cols = pl.ds(h * hd, hd)
        big.append(
            [
                pltpu.make_async_copy(w.at[:, cols], wbuf.at[h, :, pl.ds(i * hd, hd)], sem_w.at[h])
                for i, w in enumerate((wq_h, wk_h, wv_h, wz_h))
            ]
            + [pltpu.make_async_copy(st_h.at[:, h], ns_ref.at[:, h], sem_s.at[h])]
        )
    wo_in = pltpu.make_async_copy(wo_h, wo, sem_wo)
    e_in = [
        pltpu.make_async_copy(a, b.at[core], sem_small.at[1 + i])
        for i, (a, b) in enumerate([(eg_h, wg), (eu_h, wu), (ed_h, wdn)])
    ]
    units, waits = [], []
    for h in range(heads):
        units.append(big[h][:4])
        waits.append(pltpu.make_async_copy(wbuf.at[h], wbuf.at[h], sem_w.at[h]))
        if h + 1 == heads:
            units.append([wo_in])
            waits.append(wo_in)
        units.append(big[h][4:])
        waits.append(big[h][4])
    units += [e_in, [], [], []]
    for u in units[:2]:
        for c in u:
            c.start()

    def take(n):
        waits[n].wait()
        for c in units[n + 4]:
            c.start()

    z0, y0, x0 = me // (ny * nx), lax.rem(me // nx, ny), lax.rem(me, nx)
    zs = [lax.rem(z0 + i, nz) * (ny * nx) for i in range(nz)]
    ys = [lax.rem(y0 + i, ny) * nx for i in range(ny)]
    xs = [lax.rem(x0 + i, nx) for i in range(nx)]
    far, near = split_plane(ny, nx)
    count = len(far)
    ahead = lambda o: ys[o[0]] + xs[o[1]]
    behind = lambda o: ys[-o[0] % ny] + xs[-o[1] % nx]
    mine = [jnp.where(core == 1, ahead(f), ahead(n)) for f, n in zip(far, near)]
    their = [jnp.where(core == 1, ahead(n), ahead(f)) for f, n in zip(far, near)]
    home = [jnp.where(core == 1, behind(f), behind(n)) for f, n in zip(far, near)]
    hop = lambda i, n: min(i, n - i)
    order = sorted(
        [(a, j) for a in range(nz) for j in range(count)],
        key=lambda o: (-(hop(o[0], nz) + hop(far[o[1]][0], ny) + hop(far[o[1]][1], nx)), o[1] % 3, -o[0]),
    )
    order.remove((0, count - 1))
    order.append((0, count - 1))
    partner = {"ep": me, "tp": other}

    barrier = pltpu.get_barrier_semaphore()
    for a, j in order[:-1]:
        pl.semaphore_signal(barrier, inc=1, device_id={"ep": zs[a] + mine[j], "tp": core}, device_id_type=MESH)
        pl.semaphore_signal(barrier, inc=1, device_id={"ep": zs[a] + mine[j], "tp": other}, device_id_type=MESH)
        pl.semaphore_signal(barrier, inc=1, device_id={"ep": zs[a] + their[j], "tp": other}, device_id_type=MESH)
    last = zs[0] + mine[count - 1]

    @pl.when(core == 1)
    def _():
        pl.semaphore_signal(barrier, inc=1, device_id={"ep": last, "tp": core}, device_id_type=MESH)

    pl.semaphore_signal(barrier, inc=1, device_id={"ep": last, "tp": other}, device_id_type=MESH)
    pl.semaphore_signal(barrier, inc=1, device_id={"ep": zs[0] + their[count - 1], "tp": other}, device_id_type=MESH)

    for u in units[2:4]:
        for c in u:
            c.start()
    for c in small:
        c.wait()

    ids = lax.broadcasted_iota(jnp.int32, (n_ep, seqs), 0)
    row = lax.broadcasted_iota(jnp.int32, (n_ep, seqs), 1)
    r = rt[...]
    hits = [ids == r[j : j + 1, :] for j in range(2)]
    either = hits[0] | hits[1]
    first = jnp.min(jnp.where(either, row, seqs), axis=1, keepdims=True)
    final = jnp.max(jnp.where(either, row, 0), axis=1, keepdims=True)
    first_row = jnp.where(first == seqs, 0, first)
    diag = lax.broadcasted_iota(jnp.int32, (n_ep, n_ep), 0) == lax.broadcasted_iota(jnp.int32, (n_ep, n_ep), 1)
    tab_v[0:1, 0:n_ep] = jnp.sum(jnp.where(diag, first_row, 0), axis=0, keepdims=True)
    tab_v[1:2, 0:n_ep] = jnp.sum(jnp.where(diag, final, 0), axis=0, keepdims=True)
    later = jnp.where(row > first, 1, 0)
    for j in range(2):
        slot = jnp.sum(jnp.where(hits[j], later, 0), axis=0, keepdims=True)
        tab_v[2 + j : 3 + j, 0:seqs] = r[j : j + 1, :] * 2 + slot

    x = tok[...].astype(F32)
    normed = rms_scale(x, gain[...]).astype(BF16)
    normed32 = normed.astype(F32)

    def narrow(w, h):
        got = jnp.sum(normed32 * w[h : h + 1, :].astype(F32), axis=1, keepdims=True)
        return got.astype(BF16).astype(F32)

    betas = []
    for h in range(heads):
        fade = jnp.exp(-rate[h] * softplus(narrow(wd, h) + bias[h]))
        fades[h] = jnp.broadcast_to(fade, (seqs, hd))
        betas.append(jnp.broadcast_to(1.0 / (1.0 + jnp.exp(-narrow(wb, h))), (seqs, hd)))

    tab_copy = pltpu.make_async_copy(tab_v, tab, sem_small.at[0])
    tab_copy.start()

    sub = lax.broadcasted_iota(jnp.int32, (8, hd), 0)

    def project(h):
        return jnp.dot(normed, wbuf[h], preferred_element_type=F32).astype(BF16).astype(F32)

    def gates(h, raw):
        q = unit_rows(silu(raw[:, 0:hd])) * hd ** (-0.5)
        k = unit_rows(silu(raw[:, hd : 2 * hd]))
        v = silu(raw[:, 2 * hd : 3 * hd])
        z = silu(raw[:, 3 * hd : 4 * hd])
        kq = jnp.sum(k * q, axis=1, keepdims=True)
        kts[h] = k.T
        return q, k, v, z, kq

    def mixing(h, q, k, v, z, kq):
        preds, sqs = [], []
        for g in range(seqs // 8):
            both = jnp.concatenate([k[g * 8 : g * 8 + 8], q[g * 8 : g * 8 + 8]], axis=0).astype(BF16)
            pred = sq = None
            for s in range(0, 8, 2):
                two = jnp.concatenate([ns_ref[g * 8 + s, h], ns_ref[g * 8 + s + 1, h]], axis=1).astype(BF16)
                got = jnp.dot(both, two, preferred_element_type=F32)
                for i in range(2):
                    top, low = got[0:8, i * hd : (i + 1) * hd], got[8:16, i * hd : (i + 1) * hd]
                    pred = top if pred is None else jnp.where(sub == s + i, top, pred)
                    sq = low if sq is None else jnp.where(sub == s + i, low, sq)
            preds.append(pred)
            sqs.append(sq)
        pred, sq = jnp.concatenate(preds, axis=0), jnp.concatenate(sqs, axis=0)
        fade = fades[h]
        wr = betas[h] * (v - fade * pred)
        written[h] = wr
        read = fade * sq + kq * wr
        ho[:, h * hd : (h + 1) * hd] = (rms_scale(read, og[...]) * z).astype(BF16)

    early = (heads - 1) * hd
    take(0)
    raw = project(0)
    for h in range(heads - 1):
        take(2 * h + 1)
        take(2 * h + 2)
        after = project(h + 1)
        mixing(h, *gates(h, raw))
        raw = after
    take(2 * heads - 1)
    ready = gates(heads - 1, raw)
    mix32[...] = jnp.dot(ho[:, :early], wo[:early], preferred_element_type=F32)
    take(2 * heads)
    mixing(heads - 1, *ready)
    mix[...] = (mix32[...] + jnp.dot(ho[:, early:], wo[early:], preferred_element_type=F32)).astype(BF16)
    pl.semaphore_wait(barrier, 3 * nz * count - 1 + core)

    xchg = pltpu.make_async_remote_copy(
        mix, mix_in, sem_small.at[4], sem_x, device_id=partner, device_id_type=MESH
    )
    xchg.start()
    pushes = [
        pltpu.make_async_remote_copy(
            b.at[core], b.at[core], sem_small.at[5 + i], sem_pull.at[i], device_id=partner, device_id_type=MESH
        )
        for i, b in enumerate((wg, wu, wdn))
    ]
    e_in[0].wait()
    pushes[0].start()
    tab_copy.wait()
    xchg.wait()

    resid = tok[...].astype(F32) + (mix[...].astype(F32) + mix_in[...].astype(F32))
    moe_in = rms_scale(resid, fgain[...])
    for t in range(tiles):
        moe32[pl.ds(t, seqs, stride=tiles), :] = moe_in[:, t * LANES : (t + 1) * LANES]

    @pl.when(core == 0)
    def _():
        res[...] = resid[:, :half]

    @pl.when(core == 1)
    def _():
        res[...] = resid[:, half:]

    for t in range(seqs):
        moe[t] = moe32[t * tiles : (t + 1) * tiles, :].astype(BF16)
    pair = lambda i: pl.ds(2 * i, 2)
    for i, (a, j) in enumerate(order):
        for slot in range(2):
            send[2 * i + slot] = moe[tab[slot, zs[a] + mine[j]]]
    cuts = CUTS
    sem_send, sem_self, sem_back = sem_small.at[8], sem_small.at[9], sem_wo
    group = sum(jnp.where(z0 >= cut, 1, 0) for cut in cuts[1:-1])
    end = len(order) - 1
    for i, (a, j) in enumerate(order[:-1]):
        pltpu.make_async_remote_copy(
            send.at[pair(i)], recv.at[pair(z0 * count + j)], sem_send, sem_recv.at[group],
            device_id={"ep": zs[a] + mine[j], "tp": core}, device_id_type=MESH,
        ).start()
    landing = recv.at[pair(z0 * count + count - 1)]
    end_far = pltpu.make_async_remote_copy(
        send.at[pair(end)], landing, sem_self, sem_recv.at[group], device_id={"ep": last, "tp": core}, device_id_type=MESH
    )
    end_local = pltpu.make_async_copy(send.at[pair(end)], landing, sem_recv.at[group])

    @pl.when(core == 1)
    def _():
        end_far.start()

    @pl.when(core == 0)
    def _():
        end_local.start()

    for i in (1, 2):
        e_in[i].wait()
        pushes[i].start()

    for h in range(heads):
        for s in range(seqs):
            kcol = jnp.broadcast_to(kts[h, :, s : s + 1], (hd, hd))
            ns_ref[s, h] = fades[h, s : s + 1, :] * ns_ref[s, h] + kcol * written[h, s : s + 1, :]

    place = pl.ds(2 * me, 2)
    per_z = 2 * count
    locals_ = []
    for g in range(len(cuts) - 1):
        low, rows = cuts[g] * per_z, (cuts[g + 1] - cuts[g]) * per_z
        here = recv.at[pl.ds(low, rows)]
        pltpu.make_async_copy(here, here, sem_recv.at[g]).wait()
        for t in range(rows):
            rows32[t * tiles : (t + 1) * tiles, :] = recv[low + t].astype(F32)
        for t in range(tiles):
            lhs[:rows, t * LANES : (t + 1) * LANES] = rows32[pl.ds(t, rows, stride=tiles), :].astype(BF16)
        if g == 0:
            pushes[0].wait()
            pushes[1].wait()
        hid = []
        for p in range(2):
            gate = jnp.dot(lhs[:rows], wg[p], preferred_element_type=F32)
            up = jnp.dot(lhs[:rows], wu[p], preferred_element_type=F32)
            hid.append((silu(gate) * up).astype(BF16))
        if g == 0:
            pushes[2].wait()
        for hh in range(2):
            for t in range(hh * htiles, (hh + 1) * htiles):
                cols = slice(t * LANES, (t + 1) * LANES)
                got = jnp.dot(hid[0], wdn[0, :, cols], preferred_element_type=F32) + jnp.dot(
                    hid[1], wdn[1, :, cols], preferred_element_type=F32
                )
                term32[pl.ds(t, rows, stride=tiles), :] = got
            for i in range(rows // 2):
                for slot in range(2):
                    at = (2 * i + slot) * tiles + hh * htiles
                    rsend[hh, low // 2 + i, slot] = term32[at : at + htiles, :].astype(BF16)
            for j in range(count):
                for z in range(cuts[g], cuts[g + 1]):
                    d, i = z * (ny * nx) + home[j], z * count + j
                    if hh == 1 or j + 1 < count:
                        pltpu.make_async_remote_copy(
                            rsend.at[hh, i], ret.at[place], sem_back, sem_home,
                            device_id={"ep": d, "tp": hh}, device_id_type=MESH,
                        ).start()
                        continue
                    stays = (z == z0) & (core == 0)
                    back_far = pltpu.make_async_remote_copy(
                        rsend.at[hh, i], ret.at[place], sem_w.at[z], sem_home,
                        device_id={"ep": d, "tp": hh}, device_id_type=MESH,
                    )
                    back_local = pltpu.make_async_copy(rsend.at[hh, i], ret.at[place], sem_home)
                    locals_.append((stays, back_far))

                    @pl.when(stays)
                    def _():
                        back_local.start()

                    @pl.when(jnp.logical_not(stays))
                    def _():
                        back_far.start()

    sent = send.at[pl.ds(0, 2 * end)]
    pltpu.make_async_copy(sent, sent, sem_send).wait()

    @pl.when(core == 1)
    def _():
        end_far.wait_send()

    sent = rsend.at[:, pl.ds(0, nz * count - nz // 2)]
    pltpu.make_async_copy(sent, sent, sem_back).wait()
    for stays, back_far in locals_:

        @pl.when(jnp.logical_not(stays))
        def _():
            back_far.wait_send()

    pltpu.make_async_copy(ret, ret, sem_home).wait()
    for t in range(2 * n_ep):
        ret32[t] = ret[t].astype(F32)
    for t in range(seqs):
        acc = None
        for j in range(2):
            one = ret32[tab[2 + j, t]] * rw[j, t]
            acc = one if acc is None else acc + one
        acc32[t * htiles : (t + 1) * htiles, :] = acc
    for t in range(htiles):
        cols = slice(t * LANES, (t + 1) * LANES)
        out_ref[:, cols] = (res[:, cols] + acc32[pl.ds(t, seqs, stride=htiles), :]).astype(BF16)


def write_kernel(out_v, ns_v, out_h, ns_h, sem):
    parts = 4
    step = ns_v.shape[0] // parts
    copies = [pltpu.make_async_copy(out_v, out_h, sem.at[parts])] + [
        pltpu.make_async_copy(ns_v.at[pl.ds(i * step, step)], ns_h.at[pl.ds(i * step, step)], sem.at[i])
        for i in range(parts)
    ]
    for c in copies:
        c.start()
    for c in copies:
        c.wait()


HBM = pl.BlockSpec(memory_space=pltpu.HBM)
VMEM = pl.BlockSpec(memory_space=pltpu.VMEM)


def keep(a):
    return pltpu.with_memory_space_constraint(a, pltpu.HBM)


def per_device(
    dims,
    tokens, attn_gain, w_query, w_key, w_value, w_zgate, w_decay, w_beta, decay_rate, decay_bias,
    state, out_gain, w_out, ffn_gain, expert_gate, expert_up, expert_down, routes, route_weight,
):
    seqs, width = tokens.shape
    heads, hd = state.shape[1], state.shape[2]
    n_ep = lax.axis_size("ep")
    tiles = width // LANES
    hidden = expert_gate.shape[2]
    dma = pltpu.SemaphoreType.DMA
    smem, vmem = pltpu.SMEM, pltpu.VMEM

    args = (
        tokens, attn_gain.reshape(1, width), w_query, w_key, w_value, w_zgate, w_decay.T, w_beta.T, decay_rate,
        decay_bias, state, out_gain.reshape(1, hd), w_out, ffn_gain.reshape(1, width), expert_gate[0], expert_up[0],
        expert_down[0], routes.T, route_weight.T,
    )
    layer_out, new_state = pl.pallas_call(
        functools.partial(layer_kernel, n_ep, dims),
        name="layer",
        out_shape=(vmem((seqs, width // 2), BF16), vmem(state.shape, F32)),
        in_specs=[HBM] * len(args),
        out_specs=(VMEM, VMEM),
        scratch_shapes=[
            vmem((seqs, width), BF16),
            vmem((1, width), F32),
            vmem((heads, width, 4 * hd), BF16),
            vmem((heads, width), BF16),
            vmem((heads, width), BF16),
            smem((heads,), F32),
            smem((heads,), F32),
            vmem((1, hd), F32),
            vmem(w_out.shape, BF16),
            vmem((1, width), F32),
            vmem((2, seqs), jnp.int32),
            smem((2, seqs), F32),
            vmem((8, LANES), jnp.int32),
            smem((8, LANES), jnp.int32),
            vmem((heads, hd, seqs), F32),
            vmem((heads, seqs, hd), F32),
            vmem((heads, seqs, hd), F32),
            vmem((seqs, heads * hd), BF16),
            vmem((seqs, width), F32),
            vmem((2, width, hidden), BF16),
            vmem((2, width, hidden), BF16),
            vmem((2, hidden, width), BF16),
            vmem((seqs, width), BF16),
            vmem((seqs, width), BF16),
            vmem((seqs * tiles, LANES), F32),
            vmem((seqs, tiles, LANES), BF16),
            vmem((n_ep, tiles, LANES), BF16),
            vmem((n_ep, tiles, LANES), BF16),
            vmem((n_ep // 2 * tiles, LANES), F32),
            vmem((n_ep // 2, width), BF16),
            vmem((n_ep // 2 * tiles, LANES), F32),
            vmem((2, n_ep // 2, 2, tiles // 2, LANES), BF16),
            vmem((2 * n_ep, tiles // 2, LANES), BF16),
            vmem((2 * n_ep, tiles // 2, LANES), F32),
            vmem((seqs * tiles // 2, LANES), F32),
            vmem((seqs, width // 2), F32),
            dma((10,)), dma((heads,)), dma((heads,)), dma, dma, dma((3,)), dma((len(CUTS) - 1,)), dma,
        ],
        compiler_params=pltpu.CompilerParams(
            collective_id=0, has_side_effects=True, vmem_limit_bytes=40 * 2**20
        ),
    )(*[keep(a) for a in args])
    return pl.pallas_call(
        write_kernel,
        name="write",
        out_shape=(jax.ShapeDtypeStruct(layer_out.shape, BF16), jax.ShapeDtypeStruct(state.shape, F32)),
        in_specs=[VMEM, VMEM],
        out_specs=(HBM, HBM),
        scratch_shapes=[dma((5,))],
        compiler_params=pltpu.CompilerParams(vmem_limit_bytes=2**20),
    )(*[pltpu.with_memory_space_constraint(a, pltpu.VMEM) for a in (layer_out, new_state)])


def solution(mesh):
    in_specs = (
        P("ep", None), P(), P(None, "tp"), P(None, "tp"), P(None, "tp"), P(None, "tp"), P(None, "tp"), P(None, "tp"),
        P("tp"), P("tp"), P("ep", "tp", None, None), P(), P("tp", None), P(), P("ep", None, "tp"), P("ep", None, "tp"),
        P("ep", "tp", None), P("ep", None), P("ep", None),
    )
    out_specs = (P("ep", "tp"), P("ep", "tp", None, None))
    side = round(mesh.shape["ep"] ** (1 / 3))
    dims = (side, side, side)
    return jax.shard_map(
        functools.partial(per_device, dims), mesh=mesh, in_specs=in_specs, out_specs=out_specs, check_vma=False
    )
```

```python
import functools

import jax
import jax.numpy as jnp
from jax import lax
from jax.experimental import pallas as pl
from jax.experimental.pallas import tpu as pltpu
from jax.sharding import PartitionSpec as P

EPS = 1e-06
F32 = jnp.float32
BF16 = jnp.bfloat16
MESH = pl.DeviceIdType.MESH
LANES = 128


def rms_scale(rows, gain):
    return rows * lax.rsqrt(jnp.mean(rows * rows, axis=-1, keepdims=True) + EPS) * gain


def unit_rows(rows):
    return rows * lax.rsqrt(jnp.sum(rows * rows, axis=-1, keepdims=True) + EPS)


def silu(x):
    return x * (1.0 / (1.0 + jnp.exp(-x)))


def softplus(x):
    return jnp.maximum(x, 0.0) + jnp.log(1.0 + jnp.exp(-jnp.abs(x)))


def split_plane(ny, nx):
    hops = lambda o: min(o[0], ny - o[0]) + min(o[1], nx - o[1])
    back = lambda o: (-o[0] % ny, -o[1] % nx)
    every = [(b, c) for b in range(ny) for c in range(nx)]
    every.sort(key=lambda o: (-hops(o), o == back(o), min(o, back(o))))
    half = len(every) // 2
    far, near = every[:half], every[half:]
    if any(back(o) not in far for o in far):
        odd = next(o for o in far if back(o) not in far)
        own = next(o for o in near if o == back(o) and any(o))
        far[far.index(odd)], near[near.index(own)] = own, odd
    assert all(back(o) in far for o in far)
    return far, near


CUTS = (0, 1, 2, 4)


def layer_kernel(
    n_ep, dims,
    tok_h, gain_h, wq_h, wk_h, wv_h, wz_h, wd_h, wb_h, rate_h, bias_h, st_h, og_h, wo_h, fgain_h, eg_h, eu_h, ed_h, rt_h, rw_h,
    out_ref, ns_ref,
    tok, gain, wbuf, wd, wb, rate, bias, og, wo, fgain, rt, rw, tab_v, tab,
    kts, written, fades, ho, mix32, raw32,
    wg, wu, wdn, mix, mix_in, moe32, moe, send, recv, rows32, lhs, term32, rsend, ret, ret32, acc32, res,
    sem_small, sem_w, sem_s, sem_wo, sem_x, sem_pull, sem_recv, sem_home,
):
    seqs, width = tok.shape
    heads, hd = kts.shape[0], kts.shape[1]
    half = width // 2
    tiles = width // LANES
    htiles = tiles // 2
    me = lax.axis_index("ep")
    core = lax.axis_index("tp")
    other = 1 - core
    nz, ny, nx = dims

    small = [
        pltpu.make_async_copy(a, b, sem_small.at[i])
        for i, (a, b) in enumerate(
            [
                (tok_h, tok), (gain_h, gain), (wd_h, wd), (wb_h, wb), (rate_h, rate), (bias_h, bias), (og_h, og),
                (rt_h, rt), (fgain_h, fgain), (rw_h, rw),
            ]
        )
    ]
    for c in small:
        c.start()
    chunks = 4
    depth = width // chunks
    part = lambda c: pl.ds(c * depth, depth)
    s_in = [pltpu.make_async_copy(st_h.at[:, h], ns_ref.at[:, h], sem_s.at[h]) for h in range(heads)]
    wo_in = pltpu.make_async_copy(wo_h, wo, sem_wo)
    e_in = [
        pltpu.make_async_copy(a, b.at[core], sem_small.at[1 + i])
        for i, (a, b) in enumerate([(eg_h, wg), (eu_h, wu), (ed_h, wdn)])
    ]
    units, waits = [], []
    for c in range(chunks):
        units.append(
            [
                pltpu.make_async_copy(w.at[part(c)], wbuf.at[i, part(c)], sem_w.at[c])
                for i, w in enumerate((wq_h, wk_h, wv_h, wz_h))
            ]
        )
        waits.append(pltpu.make_async_copy(wbuf.at[:, part(c)], wbuf.at[:, part(c)], sem_w.at[c]))
    for c in s_in[:-1] + [wo_in] + s_in[-1:]:
        units.append([c])
        waits.append(c)
    units += [e_in, [], [], []]
    for u in units[:2]:
        for c in u:
            c.start()

    def take(n):
        waits[n].wait()
        for c in units[n + 4]:
            c.start()

    z0, y0, x0 = me // (ny * nx), lax.rem(me // nx, ny), lax.rem(me, nx)
    zs = [lax.rem(z0 + i, nz) * (ny * nx) for i in range(nz)]
    ys = [lax.rem(y0 + i, ny) * nx for i in range(ny)]
    xs = [lax.rem(x0 + i, nx) for i in range(nx)]
    far, near = split_plane(ny, nx)
    count = len(far)
    ahead = lambda o: ys[o[0]] + xs[o[1]]
    behind = lambda o: ys[-o[0] % ny] + xs[-o[1] % nx]
    mine = [jnp.where(core == 1, ahead(f), ahead(n)) for f, n in zip(far, near)]
    their = [jnp.where(core == 1, ahead(n), ahead(f)) for f, n in zip(far, near)]
    home = [jnp.where(core == 1, behind(f), behind(n)) for f, n in zip(far, near)]
    hop = lambda i, n: min(i, n - i)
    order = sorted(
        [(a, j) for a in range(nz) for j in range(count)],
        key=lambda o: (-(hop(o[0], nz) + hop(far[o[1]][0], ny) + hop(far[o[1]][1], nx)), o[1] % 3, -o[0]),
    )
    order.remove((0, count - 1))
    order.append((0, count - 1))
    partner = {"ep": me, "tp": other}

    barrier = pltpu.get_barrier_semaphore()
    for a, j in order[:-1]:
        pl.semaphore_signal(barrier, inc=1, device_id={"ep": zs[a] + mine[j], "tp": core}, device_id_type=MESH)
        pl.semaphore_signal(barrier, inc=1, device_id={"ep": zs[a] + mine[j], "tp": other}, device_id_type=MESH)
        pl.semaphore_signal(barrier, inc=1, device_id={"ep": zs[a] + their[j], "tp": other}, device_id_type=MESH)
    last = zs[0] + mine[count - 1]

    @pl.when(core == 1)
    def _():
        pl.semaphore_signal(barrier, inc=1, device_id={"ep": last, "tp": core}, device_id_type=MESH)

    pl.semaphore_signal(barrier, inc=1, device_id={"ep": last, "tp": other}, device_id_type=MESH)
    pl.semaphore_signal(barrier, inc=1, device_id={"ep": zs[0] + their[count - 1], "tp": other}, device_id_type=MESH)

    for u in units[2:4]:
        for c in u:
            c.start()
    for c in small:
        c.wait()

    ids = lax.broadcasted_iota(jnp.int32, (n_ep, seqs), 0)
    row = lax.broadcasted_iota(jnp.int32, (n_ep, seqs), 1)
    r = rt[...]
    hits = [ids == r[j : j + 1, :] for j in range(2)]
    either = hits[0] | hits[1]
    first = jnp.min(jnp.where(either, row, seqs), axis=1, keepdims=True)
    final = jnp.max(jnp.where(either, row, 0), axis=1, keepdims=True)
    first_row = jnp.where(first == seqs, 0, first)
    diag = lax.broadcasted_iota(jnp.int32, (n_ep, n_ep), 0) == lax.broadcasted_iota(jnp.int32, (n_ep, n_ep), 1)
    tab_v[0:1, 0:n_ep] = jnp.sum(jnp.where(diag, first_row, 0), axis=0, keepdims=True)
    tab_v[1:2, 0:n_ep] = jnp.sum(jnp.where(diag, final, 0), axis=0, keepdims=True)
    later = jnp.where(row > first, 1, 0)
    for j in range(2):
        slot = jnp.sum(jnp.where(hits[j], later, 0), axis=0, keepdims=True)
        tab_v[2 + j : 3 + j, 0:seqs] = r[j : j + 1, :] * 2 + slot

    x = tok[...].astype(F32)
    normed = rms_scale(x, gain[...]).astype(BF16)
    normed32 = normed.astype(F32)

    def narrow(w, h):
        got = jnp.sum(normed32 * w[h : h + 1, :].astype(F32), axis=1, keepdims=True)
        return got.astype(BF16).astype(F32)

    betas = []
    for h in range(heads):
        fade = jnp.exp(-rate[h] * softplus(narrow(wd, h) + bias[h]))
        fades[h] = jnp.broadcast_to(fade, (seqs, hd))
        betas.append(jnp.broadcast_to(1.0 / (1.0 + jnp.exp(-narrow(wb, h))), (seqs, hd)))

    tab_copy = pltpu.make_async_copy(tab_v, tab, sem_small.at[0])
    tab_copy.start()

    sub = lax.broadcasted_iota(jnp.int32, (8, hd), 0)

    def gates(h, raw):
        bits = [r[:, h * hd : (h + 1) * hd].astype(BF16).astype(F32) for r in raw]
        q = unit_rows(silu(bits[0])) * hd ** (-0.5)
        k = unit_rows(silu(bits[1]))
        v = silu(bits[2])
        z = silu(bits[3])
        kq = jnp.sum(k * q, axis=1, keepdims=True)
        kts[h] = k.T
        return q, k, v, z, kq

    def mixing(h, q, k, v, z, kq):
        preds, sqs = [], []
        for g in range(seqs // 8):
            both = jnp.concatenate([k[g * 8 : g * 8 + 8], q[g * 8 : g * 8 + 8]], axis=0).astype(BF16)
            pred = sq = None
            for s in range(0, 8, 2):
                two = jnp.concatenate([ns_ref[g * 8 + s, h], ns_ref[g * 8 + s + 1, h]], axis=1).astype(BF16)
                got = jnp.dot(both, two, preferred_element_type=F32)
                for i in range(2):
                    top, low = got[0:8, i * hd : (i + 1) * hd], got[8:16, i * hd : (i + 1) * hd]
                    pred = top if pred is None else jnp.where(sub == s + i, top, pred)
                    sq = low if sq is None else jnp.where(sub == s + i, low, sq)
            preds.append(pred)
            sqs.append(sq)
        pred, sq = jnp.concatenate(preds, axis=0), jnp.concatenate(sqs, axis=0)
        fade = fades[h]
        wr = betas[h] * (v - fade * pred)
        written[h] = wr
        read = fade * sq + kq * wr
        ho[:, h * hd : (h + 1) * hd] = (rms_scale(read, og[...]) * z).astype(BF16)

    early = (heads - 1) * hd
    for c in range(chunks):
        take(c)
        for i in range(4):
            rows = slice(c * depth, (c + 1) * depth)
            got = jnp.dot(normed[:, rows], wbuf[i, rows], preferred_element_type=F32)
            raw32[i] = got if c == 0 else raw32[i] + got
    raw = [raw32[i] for i in range(4)]
    for h in range(heads - 1):
        ready = gates(h, raw)
        take(chunks + h)
        mixing(h, *ready)
    ready = gates(heads - 1, raw)
    take(chunks + heads - 1)
    take(chunks + heads)
    mixing(heads - 1, *ready)
    mix32[...] = jnp.dot(ho[:, :early], wo[:early], preferred_element_type=F32)
    mix[...] = (mix32[...] + jnp.dot(ho[:, early:], wo[early:], preferred_element_type=F32)).astype(BF16)
    pl.semaphore_wait(barrier, 3 * nz * count - 1 + core)

    xchg = pltpu.make_async_remote_copy(
        mix, mix_in, sem_small.at[4], sem_x, device_id=partner, device_id_type=MESH
    )
    xchg.start()
    pushes = [
        pltpu.make_async_remote_copy(
            b.at[core], b.at[core], sem_small.at[5 + i], sem_pull.at[i], device_id=partner, device_id_type=MESH
        )
        for i, b in enumerate((wg, wu, wdn))
    ]
    e_in[0].wait()
    pushes[0].start()
    tab_copy.wait()
    xchg.wait()

    resid = tok[...].astype(F32) + (mix[...].astype(F32) + mix_in[...].astype(F32))
    moe_in = rms_scale(resid, fgain[...])
    for t in range(tiles):
        moe32[pl.ds(t, seqs, stride=tiles), :] = moe_in[:, t * LANES : (t + 1) * LANES]

    @pl.when(core == 0)
    def _():
        res[...] = resid[:, :half]

    @pl.when(core == 1)
    def _():
        res[...] = resid[:, half:]

    for t in range(seqs):
        moe[t] = moe32[t * tiles : (t + 1) * tiles, :].astype(BF16)
    pair = lambda i: pl.ds(2 * i, 2)
    for i, (a, j) in enumerate(order):
        for slot in range(2):
            send[2 * i + slot] = moe[tab[slot, zs[a] + mine[j]]]
    cuts = CUTS
    sem_send, sem_self, sem_back = sem_small.at[8], sem_small.at[9], sem_wo
    group = sum(jnp.where(z0 >= cut, 1, 0) for cut in cuts[1:-1])
    end = len(order) - 1
    for i, (a, j) in enumerate(order[:-1]):
        pltpu.make_async_remote_copy(
            send.at[pair(i)], recv.at[pair(z0 * count + j)], sem_send, sem_recv.at[group],
            device_id={"ep": zs[a] + mine[j], "tp": core}, device_id_type=MESH,
        ).start()
    landing = recv.at[pair(z0 * count + count - 1)]
    end_far = pltpu.make_async_remote_copy(
        send.at[pair(end)], landing, sem_self, sem_recv.at[group], device_id={"ep": last, "tp": core}, device_id_type=MESH
    )
    end_local = pltpu.make_async_copy(send.at[pair(end)], landing, sem_recv.at[group])

    @pl.when(core == 1)
    def _():
        end_far.start()

    @pl.when(core == 0)
    def _():
        end_local.start()

    for i in (1, 2):
        e_in[i].wait()
        pushes[i].start()

    for h in range(heads):
        for s in range(seqs):
            kcol = jnp.broadcast_to(kts[h, :, s : s + 1], (hd, hd))
            ns_ref[s, h] = fades[h, s : s + 1, :] * ns_ref[s, h] + kcol * written[h, s : s + 1, :]

    place = pl.ds(2 * me, 2)
    per_z = 2 * count
    locals_ = []
    for g in range(len(cuts) - 1):
        low, rows = cuts[g] * per_z, (cuts[g + 1] - cuts[g]) * per_z
        here = recv.at[pl.ds(low, rows)]
        pltpu.make_async_copy(here, here, sem_recv.at[g]).wait()
        for t in range(rows):
            rows32[t * tiles : (t + 1) * tiles, :] = recv[low + t].astype(F32)
        for t in range(tiles):
            lhs[:rows, t * LANES : (t + 1) * LANES] = rows32[pl.ds(t, rows, stride=tiles), :].astype(BF16)
        if g == 0:
            pushes[0].wait()
            pushes[1].wait()
        hid = []
        for p in range(2):
            gate = jnp.dot(lhs[:rows], wg[p], preferred_element_type=F32)
            up = jnp.dot(lhs[:rows], wu[p], preferred_element_type=F32)
            hid.append((silu(gate) * up).astype(BF16))
        if g == 0:
            pushes[2].wait()
        for hh in range(2):
            for t in range(hh * htiles, (hh + 1) * htiles):
                cols = slice(t * LANES, (t + 1) * LANES)
                got = jnp.dot(hid[0], wdn[0, :, cols], preferred_element_type=F32) + jnp.dot(
                    hid[1], wdn[1, :, cols], preferred_element_type=F32
                )
                term32[pl.ds(t, rows, stride=tiles), :] = got
            for i in range(rows // 2):
                for slot in range(2):
                    at = (2 * i + slot) * tiles + hh * htiles
                    rsend[hh, low // 2 + i, slot] = term32[at : at + htiles, :].astype(BF16)
            for j in range(count):
                for z in range(cuts[g], cuts[g + 1]):
                    d, i = z * (ny * nx) + home[j], z * count + j
                    if hh == 1 or j + 1 < count:
                        pltpu.make_async_remote_copy(
                            rsend.at[hh, i], ret.at[place], sem_back, sem_home,
                            device_id={"ep": d, "tp": hh}, device_id_type=MESH,
                        ).start()
                        continue
                    stays = (z == z0) & (core == 0)
                    back_far = pltpu.make_async_remote_copy(
                        rsend.at[hh, i], ret.at[place], sem_w.at[z], sem_home,
                        device_id={"ep": d, "tp": hh}, device_id_type=MESH,
                    )
                    back_local = pltpu.make_async_copy(rsend.at[hh, i], ret.at[place], sem_home)
                    locals_.append((stays, back_far))

                    @pl.when(stays)
                    def _():
                        back_local.start()

                    @pl.when(jnp.logical_not(stays))
                    def _():
                        back_far.start()

    sent = send.at[pl.ds(0, 2 * end)]
    pltpu.make_async_copy(sent, sent, sem_send).wait()

    @pl.when(core == 1)
    def _():
        end_far.wait_send()

    sent = rsend.at[:, pl.ds(0, nz * count - nz // 2)]
    pltpu.make_async_copy(sent, sent, sem_back).wait()
    for stays, back_far in locals_:

        @pl.when(jnp.logical_not(stays))
        def _():
            back_far.wait_send()

    pltpu.make_async_copy(ret, ret, sem_home).wait()
    for t in range(2 * n_ep):
        ret32[t] = ret[t].astype(F32)
    for t in range(seqs):
        acc = None
        for j in range(2):
            one = ret32[tab[2 + j, t]] * rw[j, t]
            acc = one if acc is None else acc + one
        acc32[t * htiles : (t + 1) * htiles, :] = acc
    for t in range(htiles):
        cols = slice(t * LANES, (t + 1) * LANES)
        out_ref[:, cols] = (res[:, cols] + acc32[pl.ds(t, seqs, stride=htiles), :]).astype(BF16)


def write_kernel(out_v, ns_v, out_h, ns_h, sem):
    parts = 4
    step = ns_v.shape[0] // parts
    copies = [pltpu.make_async_copy(out_v, out_h, sem.at[parts])] + [
        pltpu.make_async_copy(ns_v.at[pl.ds(i * step, step)], ns_h.at[pl.ds(i * step, step)], sem.at[i])
        for i in range(parts)
    ]
    for c in copies:
        c.start()
    for c in copies:
        c.wait()


HBM = pl.BlockSpec(memory_space=pltpu.HBM)
VMEM = pl.BlockSpec(memory_space=pltpu.VMEM)


def keep(a):
    return pltpu.with_memory_space_constraint(a, pltpu.HBM)


def per_device(
    dims,
    tokens, attn_gain, w_query, w_key, w_value, w_zgate, w_decay, w_beta, decay_rate, decay_bias,
    state, out_gain, w_out, ffn_gain, expert_gate, expert_up, expert_down, routes, route_weight,
):
    seqs, width = tokens.shape
    heads, hd = state.shape[1], state.shape[2]
    n_ep = lax.axis_size("ep")
    tiles = width // LANES
    hidden = expert_gate.shape[2]
    dma = pltpu.SemaphoreType.DMA
    smem, vmem = pltpu.SMEM, pltpu.VMEM

    args = (
        tokens, attn_gain.reshape(1, width), w_query, w_key, w_value, w_zgate, w_decay.T, w_beta.T, decay_rate,
        decay_bias, state, out_gain.reshape(1, hd), w_out, ffn_gain.reshape(1, width), expert_gate[0], expert_up[0],
        expert_down[0], routes.T, route_weight.T,
    )
    layer_out, new_state = pl.pallas_call(
        functools.partial(layer_kernel, n_ep, dims),
        name="layer",
        out_shape=(vmem((seqs, width // 2), BF16), vmem(state.shape, F32)),
        in_specs=[HBM] * len(args),
        out_specs=(VMEM, VMEM),
        scratch_shapes=[
            vmem((seqs, width), BF16),
            vmem((1, width), F32),
            vmem((4, width, heads * hd), BF16),
            vmem((heads, width), BF16),
            vmem((heads, width), BF16),
            smem((heads,), F32),
            smem((heads,), F32),
            vmem((1, hd), F32),
            vmem(w_out.shape, BF16),
            vmem((1, width), F32),
            vmem((2, seqs), jnp.int32),
            smem((2, seqs), F32),
            vmem((8, LANES), jnp.int32),
            smem((8, LANES), jnp.int32),
            vmem((heads, hd, seqs), F32),
            vmem((heads, seqs, hd), F32),
            vmem((heads, seqs, hd), F32),
            vmem((seqs, heads * hd), BF16),
            vmem((seqs, width), F32),
            vmem((4, seqs, heads * hd), F32),
            vmem((2, width, hidden), BF16),
            vmem((2, width, hidden), BF16),
            vmem((2, hidden, width), BF16),
            vmem((seqs, width), BF16),
            vmem((seqs, width), BF16),
            vmem((seqs * tiles, LANES), F32),
            vmem((seqs, tiles, LANES), BF16),
            vmem((n_ep, tiles, LANES), BF16),
            vmem((n_ep, tiles, LANES), BF16),
            vmem((n_ep // 2 * tiles, LANES), F32),
            vmem((n_ep // 2, width), BF16),
            vmem((n_ep // 2 * tiles, LANES), F32),
            vmem((2, n_ep // 2, 2, tiles // 2, LANES), BF16),
            vmem((2 * n_ep, tiles // 2, LANES), BF16),
            vmem((2 * n_ep, tiles // 2, LANES), F32),
            vmem((seqs * tiles // 2, LANES), F32),
            vmem((seqs, width // 2), F32),
            dma((10,)), dma((heads,)), dma((heads,)), dma, dma, dma((3,)), dma((len(CUTS) - 1,)), dma,
        ],
        compiler_params=pltpu.CompilerParams(
            collective_id=0, has_side_effects=True, vmem_limit_bytes=40 * 2**20
        ),
    )(*[keep(a) for a in args])
    return pl.pallas_call(
        write_kernel,
        name="write",
        out_shape=(jax.ShapeDtypeStruct(layer_out.shape, BF16), jax.ShapeDtypeStruct(state.shape, F32)),
        in_specs=[VMEM, VMEM],
        out_specs=(HBM, HBM),
        scratch_shapes=[dma((5,))],
        compiler_params=pltpu.CompilerParams(vmem_limit_bytes=2**20),
    )(*[pltpu.with_memory_space_constraint(a, pltpu.VMEM) for a in (layer_out, new_state)])


def solution(mesh):
    in_specs = (
        P("ep", None), P(), P(None, "tp"), P(None, "tp"), P(None, "tp"), P(None, "tp"), P(None, "tp"), P(None, "tp"),
        P("tp"), P("tp"), P("ep", "tp", None, None), P(), P("tp", None), P(), P("ep", None, "tp"), P("ep", None, "tp"),
        P("ep", "tp", None), P("ep", None), P("ep", None),
    )
    out_specs = (P("ep", "tp"), P("ep", "tp", None, None))
    side = round(mesh.shape["ep"] ** (1 / 3))
    dims = (side, side, side)
    return jax.shard_map(
        functools.partial(per_device, dims), mesh=mesh, in_specs=in_specs, out_specs=out_specs, check_vma=False
    )
```

```python
import functools

import jax
import jax.numpy as jnp
from jax import lax
from jax.experimental import pallas as pl
from jax.experimental.pallas import tpu as pltpu
from jax.sharding import PartitionSpec as P

EPS = 1e-06
F32 = jnp.float32
BF16 = jnp.bfloat16
MESH = pl.DeviceIdType.MESH
LANES = 128


def rms_scale(rows, gain):
    return rows * lax.rsqrt(jnp.mean(rows * rows, axis=-1, keepdims=True) + EPS) * gain


def unit_rows(rows):
    return rows * lax.rsqrt(jnp.sum(rows * rows, axis=-1, keepdims=True) + EPS)


def silu(x):
    return x * (1.0 / (1.0 + jnp.exp(-x)))


def softplus(x):
    return jnp.maximum(x, 0.0) + jnp.log(1.0 + jnp.exp(-jnp.abs(x)))


def split_plane(ny, nx):
    hops = lambda o: min(o[0], ny - o[0]) + min(o[1], nx - o[1])
    back = lambda o: (-o[0] % ny, -o[1] % nx)
    every = [(b, c) for b in range(ny) for c in range(nx)]
    every.sort(key=lambda o: (-hops(o), o == back(o), min(o, back(o))))
    half = len(every) // 2
    far, near = every[:half], every[half:]
    if any(back(o) not in far for o in far):
        odd = next(o for o in far if back(o) not in far)
        own = next(o for o in near if o == back(o) and any(o))
        far[far.index(odd)], near[near.index(own)] = own, odd
    assert all(back(o) in far for o in far)
    return far, near


CUTS = (0, 1, 2, 4)


def layer_kernel(
    n_ep, dims,
    tok_h, gain_h, wq_h, wk_h, wv_h, wz_h, wd_h, wb_h, rate_h, bias_h, st_h, og_h, wo_h, fgain_h, eg_h, eu_h, ed_h, rt_h, rw_h,
    out_ref, ns_ref,
    tok, gain, wbuf, wd, wb, rate, bias, og, wo, fgain, rt, rw, tab_v, tab,
    kts, written, fades, ho, mix32, raw32,
    wg, wu, wdn, mix, mix_in, moe32, moe, send, recv, rows32, lhs, term32, rsend, ret, ret32, acc32, res,
    sem_small, sem_w, sem_s, sem_wo, sem_x, sem_pull, sem_recv, sem_home,
):
    seqs, width = tok.shape
    heads, hd = kts.shape[0], kts.shape[1]
    half = width // 2
    tiles = width // LANES
    htiles = tiles // 2
    me = lax.axis_index("ep")
    core = lax.axis_index("tp")
    other = 1 - core
    nz, ny, nx = dims

    small = [
        pltpu.make_async_copy(a, b, sem_small.at[i])
        for i, (a, b) in enumerate(
            [
                (tok_h, tok), (gain_h, gain), (wd_h, wd), (wb_h, wb), (rate_h, rate), (bias_h, bias), (og_h, og),
                (rt_h, rt), (fgain_h, fgain), (rw_h, rw),
            ]
        )
    ]
    for c in small:
        c.start()
    chunks = 4
    depth = width // chunks
    part = lambda c: pl.ds(c * depth, depth)
    s_in = [pltpu.make_async_copy(st_h.at[:, h], ns_ref.at[:, h], sem_s.at[h]) for h in range(heads)]
    wo_in = pltpu.make_async_copy(wo_h, wo, sem_wo)
    e_in = [
        pltpu.make_async_copy(a, b.at[core], sem_small.at[1 + i])
        for i, (a, b) in enumerate([(eg_h, wg), (eu_h, wu), (ed_h, wdn)])
    ]
    units, waits = [], []
    for c in range(chunks):
        units.append(
            [
                pltpu.make_async_copy(w.at[part(c)], wbuf.at[i, part(c)], sem_w.at[c])
                for i, w in enumerate((wq_h, wk_h, wv_h, wz_h))
            ]
        )
        waits.append(pltpu.make_async_copy(wbuf.at[:, part(c)], wbuf.at[:, part(c)], sem_w.at[c]))
    for c in s_in[:-1] + [wo_in] + s_in[-1:]:
        units.append([c])
        waits.append(c)
    units += [[], e_in, [], []]
    for u in units[:2]:
        for c in u:
            c.start()

    def take(n):
        waits[n].wait()
        for c in units[n + 4]:
            c.start()

    z0, y0, x0 = me // (ny * nx), lax.rem(me // nx, ny), lax.rem(me, nx)
    zs = [lax.rem(z0 + i, nz) * (ny * nx) for i in range(nz)]
    ys = [lax.rem(y0 + i, ny) * nx for i in range(ny)]
    xs = [lax.rem(x0 + i, nx) for i in range(nx)]
    far, near = split_plane(ny, nx)
    count = len(far)
    ahead = lambda o: ys[o[0]] + xs[o[1]]
    behind = lambda o: ys[-o[0] % ny] + xs[-o[1] % nx]
    mine = [jnp.where(core == 1, ahead(f), ahead(n)) for f, n in zip(far, near)]
    their = [jnp.where(core == 1, ahead(n), ahead(f)) for f, n in zip(far, near)]
    home = [jnp.where(core == 1, behind(f), behind(n)) for f, n in zip(far, near)]
    hop = lambda i, n: min(i, n - i)
    order = sorted(
        [(a, j) for a in range(nz) for j in range(count)],
        key=lambda o: (-(hop(o[0], nz) + hop(far[o[1]][0], ny) + hop(far[o[1]][1], nx)), o[1] % 3, -o[0]),
    )
    order.remove((0, count - 1))
    order.append((0, count - 1))
    partner = {"ep": me, "tp": other}

    barrier = pltpu.get_barrier_semaphore()
    for a, j in order[:-1]:
        pl.semaphore_signal(barrier, inc=1, device_id={"ep": zs[a] + mine[j], "tp": core}, device_id_type=MESH)
        pl.semaphore_signal(barrier, inc=1, device_id={"ep": zs[a] + mine[j], "tp": other}, device_id_type=MESH)
        pl.semaphore_signal(barrier, inc=1, device_id={"ep": zs[a] + their[j], "tp": other}, device_id_type=MESH)
    last = zs[0] + mine[count - 1]

    @pl.when(core == 1)
    def _():
        pl.semaphore_signal(barrier, inc=1, device_id={"ep": last, "tp": core}, device_id_type=MESH)

    pl.semaphore_signal(barrier, inc=1, device_id={"ep": last, "tp": other}, device_id_type=MESH)
    pl.semaphore_signal(barrier, inc=1, device_id={"ep": zs[0] + their[count - 1], "tp": other}, device_id_type=MESH)

    for u in units[2:4]:
        for c in u:
            c.start()
    for c in small:
        c.wait()

    ids = lax.broadcasted_iota(jnp.int32, (n_ep, seqs), 0)
    row = lax.broadcasted_iota(jnp.int32, (n_ep, seqs), 1)
    r = rt[...]
    hits = [ids == r[j : j + 1, :] for j in range(2)]
    either = hits[0] | hits[1]
    first = jnp.min(jnp.where(either, row, seqs), axis=1, keepdims=True)
    final = jnp.max(jnp.where(either, row, 0), axis=1, keepdims=True)
    first_row = jnp.where(first == seqs, 0, first)
    diag = lax.broadcasted_iota(jnp.int32, (n_ep, n_ep), 0) == lax.broadcasted_iota(jnp.int32, (n_ep, n_ep), 1)
    tab_v[0:1, 0:n_ep] = jnp.sum(jnp.where(diag, first_row, 0), axis=0, keepdims=True)
    tab_v[1:2, 0:n_ep] = jnp.sum(jnp.where(diag, final, 0), axis=0, keepdims=True)
    later = jnp.where(row > first, 1, 0)
    for j in range(2):
        slot = jnp.sum(jnp.where(hits[j], later, 0), axis=0, keepdims=True)
        tab_v[2 + j : 3 + j, 0:seqs] = r[j : j + 1, :] * 2 + slot

    x = tok[...].astype(F32)
    normed = rms_scale(x, gain[...]).astype(BF16)
    normed32 = normed.astype(F32)

    def narrow(w, h):
        got = jnp.sum(normed32 * w[h : h + 1, :].astype(F32), axis=1, keepdims=True)
        return got.astype(BF16).astype(F32)

    betas = []
    for h in range(heads):
        fade = jnp.exp(-rate[h] * softplus(narrow(wd, h) + bias[h]))
        fades[h] = jnp.broadcast_to(fade, (seqs, hd))
        betas.append(jnp.broadcast_to(1.0 / (1.0 + jnp.exp(-narrow(wb, h))), (seqs, hd)))

    tab_copy = pltpu.make_async_copy(tab_v, tab, sem_small.at[0])
    tab_copy.start()

    sub = lax.broadcasted_iota(jnp.int32, (8, hd), 0)

    def gates(h, raw):
        bits = [r[:, h * hd : (h + 1) * hd].astype(BF16).astype(F32) for r in raw]
        q = unit_rows(silu(bits[0])) * hd ** (-0.5)
        k = unit_rows(silu(bits[1]))
        v = silu(bits[2])
        z = silu(bits[3])
        kq = jnp.sum(k * q, axis=1, keepdims=True)
        kts[h] = k.T
        return q, k, v, z, kq

    def mixing(h, q, k, v, z, kq):
        preds, sqs = [], []
        for g in range(seqs // 8):
            both = jnp.concatenate([k[g * 8 : g * 8 + 8], q[g * 8 : g * 8 + 8]], axis=0).astype(BF16)
            pred = sq = None
            for s in range(0, 8, 2):
                two = jnp.concatenate([ns_ref[g * 8 + s, h], ns_ref[g * 8 + s + 1, h]], axis=1).astype(BF16)
                got = jnp.dot(both, two, preferred_element_type=F32)
                for i in range(2):
                    top, low = got[0:8, i * hd : (i + 1) * hd], got[8:16, i * hd : (i + 1) * hd]
                    pred = top if pred is None else jnp.where(sub == s + i, top, pred)
                    sq = low if sq is None else jnp.where(sub == s + i, low, sq)
            preds.append(pred)
            sqs.append(sq)
        pred, sq = jnp.concatenate(preds, axis=0), jnp.concatenate(sqs, axis=0)
        fade = fades[h]
        wr = betas[h] * (v - fade * pred)
        written[h] = wr
        read = fade * sq + kq * wr
        ho[:, h * hd : (h + 1) * hd] = (rms_scale(read, og[...]) * z).astype(BF16)

    early = (heads - 1) * hd
    for c in range(chunks):
        take(c)
        for i in range(4):
            rows = slice(c * depth, (c + 1) * depth)
            got = jnp.dot(normed[:, rows], wbuf[i, rows], preferred_element_type=F32)
            raw32[i] = got if c == 0 else raw32[i] + got
    raw = [raw32[i] for i in range(4)]
    for h in range(heads - 1):
        ready = gates(h, raw)
        take(chunks + h)
        mixing(h, *ready)
    ready = gates(heads - 1, raw)
    take(chunks + heads - 1)
    mix32[...] = jnp.dot(ho[:, :early], wo[:early], preferred_element_type=F32)
    take(chunks + heads)
    mixing(heads - 1, *ready)
    mix[...] = (mix32[...] + jnp.dot(ho[:, early:], wo[early:], preferred_element_type=F32)).astype(BF16)
    pl.semaphore_wait(barrier, 3 * nz * count - 1 + core)

    xchg = pltpu.make_async_remote_copy(
        mix, mix_in, sem_small.at[4], sem_x, device_id=partner, device_id_type=MESH
    )
    xchg.start()
    pushes = [
        pltpu.make_async_remote_copy(
            b.at[core], b.at[core], sem_small.at[5 + i], sem_pull.at[i], device_id=partner, device_id_type=MESH
        )
        for i, b in enumerate((wg, wu, wdn))
    ]
    e_in[0].wait()
    pushes[0].start()
    tab_copy.wait()
    xchg.wait()

    resid = tok[...].astype(F32) + (mix[...].astype(F32) + mix_in[...].astype(F32))
    moe_in = rms_scale(resid, fgain[...])
    for t in range(tiles):
        moe32[pl.ds(t, seqs, stride=tiles), :] = moe_in[:, t * LANES : (t + 1) * LANES]

    @pl.when(core == 0)
    def _():
        res[...] = resid[:, :half]

    @pl.when(core == 1)
    def _():
        res[...] = resid[:, half:]

    for t in range(seqs):
        moe[t] = moe32[t * tiles : (t + 1) * tiles, :].astype(BF16)
    pair = lambda i: pl.ds(2 * i, 2)
    for i, (a, j) in enumerate(order):
        for slot in range(2):
            send[2 * i + slot] = moe[tab[slot, zs[a] + mine[j]]]
    cuts = CUTS
    sem_send, sem_self, sem_back = sem_small.at[8], sem_small.at[9], sem_wo
    group = sum(jnp.where(z0 >= cut, 1, 0) for cut in cuts[1:-1])
    end = len(order) - 1
    for i, (a, j) in enumerate(order[:-1]):
        pltpu.make_async_remote_copy(
            send.at[pair(i)], recv.at[pair(z0 * count + j)], sem_send, sem_recv.at[group],
            device_id={"ep": zs[a] + mine[j], "tp": core}, device_id_type=MESH,
        ).start()
    landing = recv.at[pair(z0 * count + count - 1)]
    end_far = pltpu.make_async_remote_copy(
        send.at[pair(end)], landing, sem_self, sem_recv.at[group], device_id={"ep": last, "tp": core}, device_id_type=MESH
    )
    end_local = pltpu.make_async_copy(send.at[pair(end)], landing, sem_recv.at[group])

    @pl.when(core == 1)
    def _():
        end_far.start()

    @pl.when(core == 0)
    def _():
        end_local.start()

    for i in (1, 2):
        e_in[i].wait()
        pushes[i].start()

    for h in range(heads):
        for s in range(seqs):
            kcol = jnp.broadcast_to(kts[h, :, s : s + 1], (hd, hd))
            ns_ref[s, h] = fades[h, s : s + 1, :] * ns_ref[s, h] + kcol * written[h, s : s + 1, :]

    place = pl.ds(2 * me, 2)
    per_z = 2 * count
    locals_ = []
    for g in range(len(cuts) - 1):
        low, rows = cuts[g] * per_z, (cuts[g + 1] - cuts[g]) * per_z
        here = recv.at[pl.ds(low, rows)]
        pltpu.make_async_copy(here, here, sem_recv.at[g]).wait()
        for t in range(rows):
            rows32[t * tiles : (t + 1) * tiles, :] = recv[low + t].astype(F32)
        for t in range(tiles):
            lhs[:rows, t * LANES : (t + 1) * LANES] = rows32[pl.ds(t, rows, stride=tiles), :].astype(BF16)
        if g == 0:
            pushes[0].wait()
            pushes[1].wait()
        hid = []
        for p in range(2):
            gate = jnp.dot(lhs[:rows], wg[p], preferred_element_type=F32)
            up = jnp.dot(lhs[:rows], wu[p], preferred_element_type=F32)
            hid.append((silu(gate) * up).astype(BF16))
        if g == 0:
            pushes[2].wait()
        for hh in range(2):
            for t in range(hh * htiles, (hh + 1) * htiles):
                cols = slice(t * LANES, (t + 1) * LANES)
                got = jnp.dot(hid[0], wdn[0, :, cols], preferred_element_type=F32) + jnp.dot(
                    hid[1], wdn[1, :, cols], preferred_element_type=F32
                )
                term32[pl.ds(t, rows, stride=tiles), :] = got
            for i in range(rows // 2):
                for slot in range(2):
                    at = (2 * i + slot) * tiles + hh * htiles
                    rsend[hh, low // 2 + i, slot] = term32[at : at + htiles, :].astype(BF16)
            for j in range(count):
                for z in range(cuts[g], cuts[g + 1]):
                    d, i = z * (ny * nx) + home[j], z * count + j
                    if hh == 1 or j + 1 < count:
                        pltpu.make_async_remote_copy(
                            rsend.at[hh, i], ret.at[place], sem_back, sem_home,
                            device_id={"ep": d, "tp": hh}, device_id_type=MESH,
                        ).start()
                        continue
                    stays = (z == z0) & (core == 0)
                    back_far = pltpu.make_async_remote_copy(
                        rsend.at[hh, i], ret.at[place], sem_w.at[z], sem_home,
                        device_id={"ep": d, "tp": hh}, device_id_type=MESH,
                    )
                    back_local = pltpu.make_async_copy(rsend.at[hh, i], ret.at[place], sem_home)
                    locals_.append((stays, back_far))

                    @pl.when(stays)
                    def _():
                        back_local.start()

                    @pl.when(jnp.logical_not(stays))
                    def _():
                        back_far.start()

    sent = send.at[pl.ds(0, 2 * end)]
    pltpu.make_async_copy(sent, sent, sem_send).wait()

    @pl.when(core == 1)
    def _():
        end_far.wait_send()

    sent = rsend.at[:, pl.ds(0, nz * count - nz // 2)]
    pltpu.make_async_copy(sent, sent, sem_back).wait()
    for stays, back_far in locals_:

        @pl.when(jnp.logical_not(stays))
        def _():
            back_far.wait_send()

    pltpu.make_async_copy(ret, ret, sem_home).wait()
    for t in range(2 * n_ep):
        ret32[t] = ret[t].astype(F32)
    for t in range(seqs):
        acc = None
        for j in range(2):
            one = ret32[tab[2 + j, t]] * rw[j, t]
            acc = one if acc is None else acc + one
        acc32[t * htiles : (t + 1) * htiles, :] = acc
    for t in range(htiles):
        cols = slice(t * LANES, (t + 1) * LANES)
        out_ref[:, cols] = (res[:, cols] + acc32[pl.ds(t, seqs, stride=htiles), :]).astype(BF16)


def write_kernel(out_v, ns_v, out_h, ns_h, sem):
    parts = 4
    step = ns_v.shape[0] // parts
    copies = [pltpu.make_async_copy(out_v, out_h, sem.at[parts])] + [
        pltpu.make_async_copy(ns_v.at[pl.ds(i * step, step)], ns_h.at[pl.ds(i * step, step)], sem.at[i])
        for i in range(parts)
    ]
    for c in copies:
        c.start()
    for c in copies:
        c.wait()


HBM = pl.BlockSpec(memory_space=pltpu.HBM)
VMEM = pl.BlockSpec(memory_space=pltpu.VMEM)


def keep(a):
    return pltpu.with_memory_space_constraint(a, pltpu.HBM)


def per_device(
    dims,
    tokens, attn_gain, w_query, w_key, w_value, w_zgate, w_decay, w_beta, decay_rate, decay_bias,
    state, out_gain, w_out, ffn_gain, expert_gate, expert_up, expert_down, routes, route_weight,
):
    seqs, width = tokens.shape
    heads, hd = state.shape[1], state.shape[2]
    n_ep = lax.axis_size("ep")
    tiles = width // LANES
    hidden = expert_gate.shape[2]
    dma = pltpu.SemaphoreType.DMA
    smem, vmem = pltpu.SMEM, pltpu.VMEM

    args = (
        tokens, attn_gain.reshape(1, width), w_query, w_key, w_value, w_zgate, w_decay.T, w_beta.T, decay_rate,
        decay_bias, state, out_gain.reshape(1, hd), w_out, ffn_gain.reshape(1, width), expert_gate[0], expert_up[0],
        expert_down[0], routes.T, route_weight.T,
    )
    layer_out, new_state = pl.pallas_call(
        functools.partial(layer_kernel, n_ep, dims),
        name="layer",
        out_shape=(vmem((seqs, width // 2), BF16), vmem(state.shape, F32)),
        in_specs=[HBM] * len(args),
        out_specs=(VMEM, VMEM),
        scratch_shapes=[
            vmem((seqs, width), BF16),
            vmem((1, width), F32),
            vmem((4, width, heads * hd), BF16),
            vmem((heads, width), BF16),
            vmem((heads, width), BF16),
            smem((heads,), F32),
            smem((heads,), F32),
            vmem((1, hd), F32),
            vmem(w_out.shape, BF16),
            vmem((1, width), F32),
            vmem((2, seqs), jnp.int32),
            smem((2, seqs), F32),
            vmem((8, LANES), jnp.int32),
            smem((8, LANES), jnp.int32),
            vmem((heads, hd, seqs), F32),
            vmem((heads, seqs, hd), F32),
            vmem((heads, seqs, hd), F32),
            vmem((seqs, heads * hd), BF16),
            vmem((seqs, width), F32),
            vmem((4, seqs, heads * hd), F32),
            vmem((2, width, hidden), BF16),
            vmem((2, width, hidden), BF16),
            vmem((2, hidden, width), BF16),
            vmem((seqs, width), BF16),
            vmem((seqs, width), BF16),
            vmem((seqs * tiles, LANES), F32),
            vmem((seqs, tiles, LANES), BF16),
            vmem((n_ep, tiles, LANES), BF16),
            vmem((n_ep, tiles, LANES), BF16),
            vmem((n_ep // 2 * tiles, LANES), F32),
            vmem((n_ep // 2, width), BF16),
            vmem((n_ep // 2 * tiles, LANES), F32),
            vmem((2, n_ep // 2, 2, tiles // 2, LANES), BF16),
            vmem((2 * n_ep, tiles // 2, LANES), BF16),
            vmem((2 * n_ep, tiles // 2, LANES), F32),
            vmem((seqs * tiles // 2, LANES), F32),
            vmem((seqs, width // 2), F32),
            dma((10,)), dma((heads,)), dma((heads,)), dma, dma, dma((3,)), dma((len(CUTS) - 1,)), dma,
        ],
        compiler_params=pltpu.CompilerParams(
            collective_id=0, has_side_effects=True, vmem_limit_bytes=40 * 2**20
        ),
    )(*[keep(a) for a in args])
    return pl.pallas_call(
        write_kernel,
        name="write",
        out_shape=(jax.ShapeDtypeStruct(layer_out.shape, BF16), jax.ShapeDtypeStruct(state.shape, F32)),
        in_specs=[VMEM, VMEM],
        out_specs=(HBM, HBM),
        scratch_shapes=[dma((5,))],
        compiler_params=pltpu.CompilerParams(vmem_limit_bytes=2**20),
    )(*[pltpu.with_memory_space_constraint(a, pltpu.VMEM) for a in (layer_out, new_state)])


def solution(mesh):
    in_specs = (
        P("ep", None), P(), P(None, "tp"), P(None, "tp"), P(None, "tp"), P(None, "tp"), P(None, "tp"), P(None, "tp"),
        P("tp"), P("tp"), P("ep", "tp", None, None), P(), P("tp", None), P(), P("ep", None, "tp"), P("ep", None, "tp"),
        P("ep", "tp", None), P("ep", None), P("ep", None),
    )
    out_specs = (P("ep", "tp"), P("ep", "tp", None, None))
    side = round(mesh.shape["ep"] ** (1 / 3))
    dims = (side, side, side)
    return jax.shard_map(
        functools.partial(per_device, dims), mesh=mesh, in_specs=in_specs, out_specs=out_specs, check_vma=False
    )
```
